32 devices in a mesh: ep: 8 (over z, x), tp: 4 (over y, core).
Axes of the slice: x: 2, y: 2, z: 4, core: 2. Of those that a mesh axis runs over, the one named last changes fastest.
Arguments:
- query_latent: bfloat16 [1024, 512], P('ep'), may hold values from -6 to 6
- key_latent: bfloat16 [1024, 256], P('ep'), may hold values from -6 to 6
- rope_key: bfloat16 [1024, 64], P('ep'), may hold values from -500 to 500
- query_gain: float32 [512], replicated, may hold values from 0.1 to 1.9
- key_gain: float32 [256], replicated, may hold values from 0.1 to 1.9
- w_query: bfloat16 [512, 1024], P(None, 'tp'), may hold values from -0.25 to 0.25
- w_query_rope: bfloat16 [512, 512], P(None, 'tp'), may hold values from -0.25 to 0.25
- w_key: bfloat16 [256, 1024], P(None, 'tp'), may hold values from -0.375 to 0.375
- w_value: bfloat16 [256, 1024], P(None, 'tp'), may hold values from -0.375 to 0.375
- w_out: bfloat16 [1024, 2048], P('tp'), may hold values from -1.796875 to 1.796875
- tokens_b: bfloat16 [4096, 2048], P('ep'), may hold values from -6 to 6
- ffn_gain: float32 [2048], replicated, may hold values from 0.1 to 1.9
- route_expert: int32 [4096, 2], P('ep'), may hold values from 0 to 7, as said below
- route_weight: float32 [4096, 2], P('ep'), may hold values from 0.2 to 1
- w_gate: bfloat16 [8, 2048, 1024], P('ep', None, 'tp'), may hold values from -0.125 to 0.125
- w_up: bfloat16 [8, 2048, 1024], P('ep', None, 'tp'), may hold values from -0.125 to 0.125
- w_down: bfloat16 [8, 1024, 2048], P('ep', 'tp'), may hold values from -0.1875 to 0.1875
Outputs:
- mixer_out: bfloat16 [1024, 2048], P(('ep', 'tp'))
- moe_out: bfloat16 [4096, 2048], P('ep', 'tp')
The draws below stay inside these ranges and needn't reach their ends.
Inputs may be any that keep to these rules, and one draw needn't show every extreme that they name: `route_expert`: expert e belongs to group e // 2. A row's 2 experts differ and lie in one group. Among the rows of one device along ep, every group is named by exactly 128 rows and every expert is named exactly 128 times.
All inputs are finite; a program needn't handle non-finite values.
Results may differ from the reference program's by a relative error of at most 0.013.
The reference program's roundings to bfloat16 on the way count: a program that leaves them out, or rounds other values in their place, can miss the bound.
Values may be sent and summed in bfloat16 or wider, within the bound.
A program may use at most 64 MiB of HBM per device.

```python
import math
import jax
import jax.numpy as jnp
from jax import lax

D = 2048
HEADS = 8
NOPE = 128
ROPE = 64
VDIM = 128
QRANK = 512
KVRANK = 256
GRID_W = 64
FF_E = 1024
GROUPS = 4
TOPK = 2
TOK_A = 128
TOK_B = 512
EXPERTS = 8
TOKENS_A = 1024
TOKENS_B = 4096
N_EP = 8
N_TP = 4


def draw_rope_key(key, part):
    seq_len = TOK_A * N_EP
    key_base = jax.random.fold_in(key, 0)
    return jnp.clip(3.0 * jax.random.normal(key_base, (seq_len, ROPE), jnp.float32), -18.0, 18.0).astype(jnp.bfloat16)


def draw_route_expert(key, part):
    group_rows = TOK_B // GROUPS
    in_group = EXPERTS // GROUPS
    key_order, key_rotation, key_shift = jax.random.split(key, 3)
    ranking = jax.random.randint(key_order, (N_EP, TOK_B), 0, 1 << 16) * TOK_B + jnp.arange(TOK_B, dtype=jnp.int32)[None, :]
    ordering = jnp.argsort(ranking, axis=1, stable=True)
    position = jnp.argsort(ordering, axis=1, stable=True).astype(jnp.int32)
    group_of = position // group_rows
    within = position % group_rows
    rotation = jax.random.randint(key_rotation, (N_EP, GROUPS), 0, in_group)
    shifted = jax.random.randint(key_shift, (N_EP, GROUPS), 1, in_group)
    rotation_row = jnp.take_along_axis(rotation, group_of, axis=1)
    shift_row = jnp.take_along_axis(shifted, group_of, axis=1)
    first_choice = group_of * in_group + (within + rotation_row) % in_group
    second_choice = group_of * in_group + (within + rotation_row + shift_row) % in_group
    routes = jnp.stack([first_choice, second_choice], axis=-1)
    return routes.reshape(N_EP * TOK_B, TOPK).astype(jnp.int32)


def levels(key, extent, pieces, smallest, top_value):
    loudness = 1.0
    for dim, shards_of in pieces:
        draws = jax.random.uniform(jax.random.fold_in(jax.random.fold_in(key, 6), dim), (shards_of,), jnp.float32, smallest / len(pieces), top_value / len(pieces))
        loudness = loudness * jnp.repeat(jnp.exp(draws), extent[dim] // shards_of).reshape((-1,) + (1,) * (len(extent) - 1 - dim))
    return loudness


def noise(stream_key, shape, deviation, most, cuts=(), held_as=jnp.bfloat16):
    values = jax.random.normal(stream_key, shape, jnp.float32) * deviation
    if len(cuts) > 0:
        values = levels(stream_key, shape, cuts, -0.22, 0.18) * values
    return jnp.clip(values, min=-most, max=most).astype(held_as)


def setup_inputs(seed: int = 0) -> dict:
    key_of = jax.random.split(jax.random.key(seed), 18)
    query_latent = noise(key_of[0], (TOKENS_A, QRANK), 1.0, 6.0, ((0, 8),))
    key_latent = noise(key_of[1], (TOKENS_A, KVRANK), 1.0, 6.0, ((0, 8),))
    rope_key = draw_rope_key(jax.random.fold_in(key_of[17], 71), 0)
    query_gain = jnp.clip(1.0 + 0.18 * jax.random.normal(key_of[3], (QRANK,), jnp.float32), 0.1, 1.9)
    key_gain = jnp.clip(1.0 + 0.18 * jax.random.normal(key_of[4], (KVRANK,), jnp.float32), 0.1, 1.9)
    w_query = noise(key_of[5], (QRANK, HEADS * NOPE), QRANK ** -0.5, 0.25, ((1, 4),))
    w_query_rope = noise(key_of[6], (QRANK, HEADS * ROPE), QRANK ** -0.5, 0.25, ((1, 4),))
    w_key = noise(key_of[7], (KVRANK, HEADS * NOPE), KVRANK ** -0.5, 0.375, ((1, 4),))
    w_value = noise(key_of[8], (KVRANK, HEADS * VDIM), KVRANK ** -0.5, 0.375, ((1, 4),))
    w_out = noise(key_of[9], (HEADS * VDIM, D), 0.3, 1.796875, ((0, 4),))
    tokens_b = noise(key_of[10], (TOKENS_B, D), 1.0, 6.0, ((0, 8),))
    ffn_gain = jnp.clip(1.0 + 0.18 * jax.random.normal(key_of[11], (D,), jnp.float32), 0.1, 1.9)
    route_expert = draw_route_expert(jax.random.fold_in(key_of[17], 71), 0)
    route_weight = jnp.clip(jnp.exp(math.log(1.0) - 1.609438 * jax.random.uniform(key_of[13], (TOKENS_B, TOPK), jnp.float32) ** levels(key_of[13], (TOKENS_B, TOPK), ((0, 8),), -0.2, 0.2)), 0.2, 1.0)
    w_gate = noise(key_of[14], (EXPERTS, D, FF_E), D ** -0.5, 0.125, ((0, 8), (2, 4)))
    w_up = noise(key_of[15], (EXPERTS, D, FF_E), D ** -0.5, 0.125, ((0, 8), (2, 4)))
    w_down = noise(key_of[16], (EXPERTS, FF_E, D), FF_E ** -0.5, 0.1875, ((0, 8), (1, 4)))
    return {"query_latent": query_latent, "key_latent": key_latent, "rope_key": rope_key, "query_gain": query_gain, "key_gain": key_gain, "w_query": w_query, "w_query_rope": w_query_rope, "w_key": w_key, "w_value": w_value, "w_out": w_out, "tokens_b": tokens_b, "ffn_gain": ffn_gain, "route_expert": route_expert, "route_weight": route_weight, "w_gate": w_gate, "w_up": w_up, "w_down": w_down}


epsilon = 1e-06
rotary_base = 10000.0

def rms_scale(values_in, gain):
    widened = values_in.astype(jnp.float32)
    normed = widened * lax.rsqrt(lax.optimization_barrier(jnp.mean(widened * widened, axis=-1, keepdims=True)) + epsilon)
    return (normed * gain.astype(jnp.float32)).astype(jnp.bfloat16)

def rotary_tables(positions):
    half_width = ROPE // 2
    inverse = rotary_base ** (-jnp.arange(0, half_width, 2, dtype=jnp.float32) / half_width)
    grid_row = (positions // GRID_W).astype(jnp.float32)
    grid_col = (positions % GRID_W).astype(jnp.float32)
    angle = jnp.concatenate([grid_row[:, None] * inverse, grid_col[:, None] * inverse], axis=-1)
    return (jnp.cos(angle), jnp.sin(angle))

def rotate(values_in, cosine, sine):
    even_part = values_in[..., 0::2]
    odd_part = values_in[..., 1::2]
    turned = jnp.stack([even_part * cosine - odd_part * sine, even_part * sine + odd_part * cosine], axis=-1)
    return turned.reshape(values_in.shape)

def mixer_half(query_latent, key_latent, rope_key, query_gain, key_gain, w_query, w_query_rope, w_key, w_value, w_out):
    seq_len = query_latent.shape[0]
    positions = jnp.arange(seq_len, dtype=jnp.int32)
    cosine, sine = rotary_tables(positions)
    query_normed = rms_scale(query_latent, query_gain)
    query_nope = jnp.dot(query_normed, w_query, preferred_element_type=jnp.float32).astype(jnp.bfloat16)
    query_nope = query_nope.reshape(seq_len, HEADS, NOPE)
    query_rot = jnp.dot(query_normed, w_query_rope, preferred_element_type=jnp.float32).reshape(seq_len, HEADS, ROPE)
    query_rot = rotate(query_rot, cosine[:, None, :], sine[:, None, :]).astype(jnp.bfloat16)
    key_normed = rms_scale(key_latent, key_gain)
    key_nope = jnp.dot(key_normed, w_key, preferred_element_type=jnp.float32).astype(jnp.bfloat16)
    key_nope = key_nope.reshape(seq_len, HEADS, NOPE)
    value_rows = jnp.dot(key_normed, w_value, preferred_element_type=jnp.float32).astype(jnp.bfloat16)
    value_rows = value_rows.reshape(seq_len, HEADS, VDIM)
    key_rot = rotate(rope_key.astype(jnp.float32), cosine, sine).astype(jnp.bfloat16)
    score_scale = (NOPE + ROPE) ** (-0.5)
    block_rows = math.gcd(seq_len, 512)

    def one_head(operands):
        head_query, head_rot, head_key, head_value = operands

        def one_block(block_operands):
            block_query, block_rot = block_operands
            scores = jnp.dot(block_query, head_key.T, preferred_element_type=jnp.float32)
            scores = (scores + jnp.dot(block_rot, key_rot.T, preferred_element_type=jnp.float32)) * score_scale
            row_max = lax.optimization_barrier(jnp.max(scores, axis=-1, keepdims=True))
            weights = jnp.exp(scores - row_max)
            totals = lax.optimization_barrier(jnp.sum(weights, axis=-1, keepdims=True))
            mixed = jnp.dot(weights.astype(jnp.bfloat16), head_value, preferred_element_type=jnp.float32)
            return (mixed / totals).astype(jnp.bfloat16)
        blocks = lax.map(one_block, (head_query.reshape(seq_len // block_rows, block_rows, NOPE), head_rot.reshape(seq_len // block_rows, block_rows, ROPE)))
        return blocks.reshape(seq_len, VDIM)
    heads_out = lax.map(one_head, (jnp.moveaxis(query_nope, 1, 0), jnp.moveaxis(query_rot, 1, 0), jnp.moveaxis(key_nope, 1, 0), jnp.moveaxis(value_rows, 1, 0)))
    heads_flat = jnp.moveaxis(heads_out, 0, 1).reshape(seq_len, HEADS * VDIM)
    group_cols = HEADS * VDIM // N_TP
    summed = jnp.zeros((seq_len, D), jnp.float32)
    for group_index in range(N_TP):
        lower = group_index * group_cols
        piece_sum = jnp.dot(heads_flat[:, lower:lower + group_cols], w_out[lower:lower + group_cols], preferred_element_type=jnp.float32).astype(jnp.bfloat16)
        summed = summed + lax.optimization_barrier(piece_sum).astype(jnp.float32)
    return summed.astype(jnp.bfloat16)

def expert_half(tokens_b, ffn_gain, route_expert, route_weight, w_gate, w_up, w_down):
    all_rows = tokens_b.shape[0]
    capacity = TOPK * TOK_B // EXPERTS
    normed = rms_scale(tokens_b, ffn_gain)
    copies = route_expert.reshape(N_EP, TOK_B * TOPK)
    expert_ids = jnp.arange(EXPERTS, dtype=jnp.int32)

    def block_slots(block_copies):
        chosen = (block_copies[:, None] == expert_ids[None, :]).astype(jnp.int32)
        earlier = jnp.cumsum(chosen, axis=0) - chosen
        return lax.optimization_barrier(jnp.sum(earlier * chosen, axis=1)).astype(jnp.int32)
    slot_index = lax.map(block_slots, copies)
    block_ids = jnp.arange(N_EP, dtype=jnp.int32)[:, None]
    target = (copies * (N_EP * capacity) + block_ids * capacity + slot_index).reshape(-1).astype(jnp.int32)
    source_row = jnp.zeros((EXPERTS * N_EP * capacity,), jnp.int32).at[target].set(jnp.arange(all_rows * TOPK, dtype=jnp.int32) // TOPK)
    source_row = source_row.reshape(EXPERTS, N_EP * capacity)
    unit_cols = FF_E // N_TP

    def one_expert(operands):
        row_ids, gate_weight, up_weight, down_weight = operands
        arrived = jnp.take(normed, row_ids, axis=0)
        gate_act = jnp.dot(arrived, gate_weight, preferred_element_type=jnp.float32)
        up_act = jnp.dot(arrived, up_weight, preferred_element_type=jnp.float32)
        hidden = (jax.nn.silu(gate_act) * up_act).astype(jnp.bfloat16)
        summed = jnp.zeros((arrived.shape[0], D), jnp.float32)
        for group_index in range(N_TP):
            lower = group_index * unit_cols
            piece_sum = jnp.dot(hidden[:, lower:lower + unit_cols], down_weight[lower:lower + unit_cols], preferred_element_type=jnp.float32).astype(jnp.bfloat16)
            summed = summed + lax.optimization_barrier(piece_sum).astype(jnp.float32)
        return summed.astype(jnp.bfloat16)
    results = lax.map(one_expert, (source_row, w_gate, w_up, w_down)).reshape(EXPERTS * N_EP * capacity, D)
    picked = jnp.take(results, target, axis=0).reshape(all_rows, TOPK, D)
    combined = lax.optimization_barrier(jnp.sum(picked.astype(jnp.float32) * route_weight[:, :, None], axis=1))
    return combined.astype(jnp.bfloat16)

def reference(query_latent, key_latent, rope_key, query_gain, key_gain, w_query, w_query_rope, w_key, w_value, w_out, tokens_b, ffn_gain, route_expert, route_weight, w_gate, w_up, w_down):
    mixer_out = mixer_half(query_latent, key_latent, rope_key, query_gain, key_gain, w_query, w_query_rope, w_key, w_value, w_out)
    moe_out = expert_half(tokens_b, ffn_gain, route_expert, route_weight, w_gate, w_up, w_down)
    return (mixer_out, moe_out)
```

```python
import functools
import math

import jax
import jax.numpy as jnp
from jax import lax
from jax.experimental import pallas as pl
from jax.experimental.pallas import tpu as pltpu
from jax.sharding import PartitionSpec as P

NOPE = 128
ROPE = 64
VDIM = 128
GRID_W = 64
TOPK = 2
GROUPS = 4
MESH = pl.DeviceIdType.MESH
HALVES = 2
SPARES = (4, 1, 4, 3, 3, 4, 4, 4)
X_LEADS = (0, 2, 3, 5, 7)
SENDS = (2, 0, 1, 6, 3, 7, 4, 5)


epsilon = 1e-06
rotary_base = 10000.0
neg_large = -1e30


def rms_scale(values_in, gain):
    widened = values_in.astype(jnp.float32)
    normed = widened * lax.rsqrt(jnp.mean(widened * widened, axis=-1, keepdims=True) + epsilon)
    return (normed * gain).astype(jnp.bfloat16)


def rotary_tables(positions):
    half_width = ROPE // 2
    inverse = rotary_base ** (-jnp.arange(0, half_width, 2, dtype=jnp.float32) / half_width)
    grid_row = (positions // GRID_W).astype(jnp.float32)
    grid_col = (positions % GRID_W).astype(jnp.float32)
    angle = jnp.concatenate([grid_row[:, None] * inverse, grid_col[:, None] * inverse], axis=-1)
    return (jnp.cos(angle), jnp.sin(angle))


def rotate(values_in, cosine, sine):
    even_part = values_in[..., 0::2]
    odd_part = values_in[..., 1::2]
    turned = jnp.stack(
        [even_part * cosine - odd_part * sine, even_part * sine + odd_part * cosine], axis=-1
    )
    return turned.reshape(values_in.shape)


def fold_blocks(carry, members, step_fn):
    piece_rows = members[0].shape[0]
    block_rows = math.gcd(piece_rows, 1024)
    if block_rows == piece_rows:
        return step_fn(carry, members)
    stacked = tuple(
        (
            member.reshape((piece_rows // block_rows, block_rows) + member.shape[1:])
            for member in members
        )
    )

    def scan_step(inner_carry, blocks):
        return (step_fn(inner_carry, blocks), None)

    result, unused = lax.scan(scan_step, carry, stacked)
    return result


def mixer_half(
    query_latent,
    key_latent,
    rope_key,
    query_gain,
    key_gain,
    w_query,
    w_query_rope,
    w_key,
    w_value,
    w_out,
):
    tok_rows = query_latent.shape[0]
    local_heads = w_query.shape[1] // NOPE
    positions = lax.axis_index("ep") * tok_rows + jnp.arange(tok_rows, dtype=jnp.int32)
    cosine, sine = rotary_tables(positions)
    query_normed = rms_scale(query_latent, query_gain)
    query_nope = jnp.dot(query_normed, w_query, preferred_element_type=jnp.float32).astype(
        jnp.bfloat16
    )
    query_nope = query_nope.reshape(tok_rows, local_heads, NOPE)
    query_rot = jnp.dot(query_normed, w_query_rope, preferred_element_type=jnp.float32)
    query_rot = rotate(
        query_rot.reshape(tok_rows, local_heads, ROPE), cosine[:, None, :], sine[:, None, :]
    )
    query_rot = query_rot.astype(jnp.bfloat16)
    key_rot = rotate(rope_key.astype(jnp.float32), cosine, sine).astype(jnp.bfloat16)
    score_scale = (NOPE + ROPE) ** (-0.5)

    def expand(latent_rows):
        latent_count = latent_rows.shape[0]
        key_normed = rms_scale(latent_rows, key_gain)
        key_nope = jnp.dot(key_normed, w_key, preferred_element_type=jnp.float32).astype(
            jnp.bfloat16
        )
        value_rows = jnp.dot(key_normed, w_value, preferred_element_type=jnp.float32).astype(
            jnp.bfloat16
        )
        return (
            key_nope.reshape(latent_count, local_heads, NOPE),
            value_rows.reshape(latent_count, local_heads, VDIM),
        )

    def attend_block(carry, key_nope, value_rows, key_turn):
        run_max, run_total, run_acc = carry
        scores = jnp.einsum(
            "qhd,khd->hqk", query_nope, key_nope, preferred_element_type=jnp.float32
        )
        scores = scores + jnp.einsum(
            "qhd,kd->hqk", query_rot, key_turn, preferred_element_type=jnp.float32
        )
        scores = scores * score_scale
        new_max = jnp.maximum(run_max, jnp.max(scores, axis=-1))
        correction = jnp.exp(run_max - new_max)
        weights = jnp.exp(scores - new_max[..., None])
        new_total = run_total * correction + jnp.sum(weights, axis=-1)
        added = jnp.einsum(
            "hqk,khd->qhd",
            weights.astype(jnp.bfloat16),
            value_rows,
            preferred_element_type=jnp.float32,
        )
        new_acc = run_acc * jnp.transpose(correction)[..., None] + added
        return (new_max, new_total, new_acc)

    def step_latent(carry, blocks):
        key_nope, value_rows = expand(blocks[0])
        return attend_block(carry, key_nope, value_rows, blocks[1])

    initial = (
        jnp.full((local_heads, tok_rows), neg_large, jnp.float32),
        jnp.zeros((local_heads, tok_rows), jnp.float32),
        jnp.zeros((tok_rows, local_heads, VDIM), jnp.float32),
    )
    gathered = lax.all_gather(
        jnp.concatenate([key_latent, key_rot], axis=1), "ep", axis=0, tiled=True
    )
    rank = key_latent.shape[1]
    final = fold_blocks(initial, (gathered[:, :rank], gathered[:, rank:]), step_latent)
    run_max, run_total, run_acc = final
    heads_out = (run_acc / jnp.transpose(run_total)[..., None]).astype(jnp.bfloat16)
    heads_out = heads_out.reshape(tok_rows, local_heads * VDIM)
    return lax.psum_scatter(
        jnp.dot(heads_out, w_out, preferred_element_type=jnp.float32).astype(jnp.bfloat16),
        "tp",
        scatter_dimension=0,
        tiled=True,
    )


def expert_half(tokens_b, ffn_gain, route_expert, route_weight, w_gate, w_up, w_down):
    tok_rows = tokens_b.shape[0]
    expert_count = lax.axis_size("ep")
    capacity = TOPK * tok_rows // expert_count
    normed = rms_scale(tokens_b, ffn_gain)
    copies = route_expert.reshape(tok_rows * TOPK)
    chosen = (copies[:, None] == jnp.arange(expert_count, dtype=jnp.int32)[None, :]).astype(
        jnp.int32
    )
    earlier = jnp.cumsum(chosen, axis=0) - chosen
    slot_index = jnp.sum(earlier * chosen, axis=1)
    target = copies * capacity + slot_index
    source_row = (
        jnp.zeros((expert_count * capacity,), jnp.int32)
        .at[target]
        .set(jnp.arange(tok_rows * TOPK, dtype=jnp.int32) // TOPK)
    )
    outgoing = jnp.take(normed, source_row, axis=0)
    share_cols = outgoing.shape[1] // lax.axis_size("tp")
    own_cols = lax.dynamic_slice_in_dim(outgoing, lax.axis_index("tp") * share_cols, share_cols, 1)
    arrived = lax.all_to_all(own_cols, "ep", split_axis=0, concat_axis=0, tiled=True)
    member = lax.all_gather(arrived, "tp", axis=1, tiled=True)
    gate_rows = w_gate[0]
    up_rows = w_up[0]
    gate_act = jnp.dot(member, gate_rows, preferred_element_type=jnp.float32)
    up_act = jnp.dot(member, up_rows, preferred_element_type=jnp.float32)
    hidden = (jax.nn.silu(gate_act) * up_act).astype(jnp.bfloat16)
    partial_term = jnp.dot(hidden, w_down[0], preferred_element_type=jnp.float32)
    shared = lax.psum_scatter(
        partial_term.astype(jnp.bfloat16), "tp", scatter_dimension=1, tiled=True
    )
    returned = lax.all_to_all(shared, "ep", split_axis=0, concat_axis=0, tiled=True)
    picked = (
        jnp.take(returned, target, axis=0)
        .astype(jnp.float32)
        .reshape(tok_rows, TOPK, returned.shape[1])
    )
    combined = jnp.sum(picked * route_weight[:, :, None], axis=1)
    return combined.astype(jnp.bfloat16)


def flip(index, distance):
    low = index % 2
    high = index // 2
    if distance % 2 == 1:
        low = 1 - low
    if distance // 2 == 1:
        high = 1 - high
    return high * 2 + low


def expert_kernel(
    tokens_hbm,
    gain_hbm,
    route_hbm,
    weight_hbm,
    gate_hbm,
    up_hbm,
    down_hbm,
    query_hbm,
    latent_hbm,
    rope_hbm,
    query_gain_hbm,
    key_gain_hbm,
    w_query_hbm,
    w_rope_hbm,
    w_key_hbm,
    w_value_hbm,
    w_out_hbm,
    moe_ref,
    mixer_ref,
    tokens_ref,
    gain_ref,
    route_ref,
    share_ref,
    query_ref,
    latent_ref,
    rope_ref,
    query_gain_ref,
    key_gain_ref,
    w_query_ref,
    w_rope_ref,
    w_key_ref,
    w_value_ref,
    w_out_ref,
    order_ref,
    back_ref,
    weight_ref,
    weight_in,
    column_ref,
    scale_ref,
    outgoing_ref,
    member_ref,
    gate_ref,
    up_ref,
    down_ref,
    pair_send,
    pair_keep,
    pair_recv,
    first_send,
    first_keep,
    first_recv,
    second_send,
    second_keep,
    second_recv,
    fin_send,
    fin_ref,
    keys_ref,
    turns_ref,
    query_nope_ref,
    query_turn_ref,
    heads_ref,
    mixed_ref,
    mixed_in,
    joint_send,
    joint_recv,
    token_sem,
    load_sem,
    z_send,
    z_recv,
    x_send,
    x_recv,
    y_send,
    y_recv,
    c_send,
    c_recv,
    p_send,
    p_recv,
    f_send,
    f_recv,
    s_send,
    s_recv,
    o_send,
    o_recv,
    w_send,
    w_recv,
    kz_send,
    kz_recv,
    kx_send,
    kx_recv,
    kc_send,
    kc_recv,
    a_send,
    a_recv,
    j_send,
    j_recv,
):
    ep = lax.axis_index("ep")
    tp = lax.axis_index("tp")
    z, x = ep // 2, ep % 2
    y, c = tp // 2, tp % 2
    rows, half = outgoing_ref.shape[1:]
    lines_of = rows // HALVES
    tok_rows = tokens_ref.shape[0]
    share = fin_ref.shape[2]

    def spare_of(u):
        return half * SPARES[u] // 8

    def carried(u):
        return pl.ds(pl.multiple_of(y * spare_of(u), 128), half - spare_of(u))

    def passed(u):
        return pl.ds(pl.multiple_of(y * (half - spare_of(u)), 128), spare_of(u))

    at_end = (z == 0) | (z == GROUPS - 1)

    def at_z(distance):
        return {"ep": flip(z, distance) * 2 + x, "tp": tp}

    at_x = {"ep": z * 2 + 1 - x, "tp": tp}
    at_y = {"ep": ep, "tp": (1 - y) * 2 + c}
    at_c = {"ep": ep, "tp": y * 2 + 1 - c}

    barrier = pltpu.get_barrier_semaphore()
    for peer in (at_z(1), at_z(2), at_z(3), at_x, at_y, at_c):
        pl.semaphore_signal(barrier, inc=1, device_id=peer, device_id_type=MESH)

    loads = {}

    def load(name, source, target):
        loads[name] = pltpu.make_async_copy(source, target, load_sem.at[len(loads)])
        loads[name].start()

    load("route", route_hbm, route_ref)
    load("gain", gain_hbm, gain_ref)
    token_loads = []
    for k in range(4):
        lines = pl.ds(k * (tok_rows // 4), tok_rows // 4)
        token_loads.append(
            pltpu.make_async_copy(tokens_hbm.at[lines], tokens_ref.at[lines], token_sem.at[k])
        )
        token_loads[k].start()
    load("share", weight_hbm, share_ref)
    load("key_gain", key_gain_hbm, key_gain_ref)
    load("latent", latent_hbm, latent_ref)
    load("rope", rope_hbm, rope_ref)
    load("gate", gate_hbm.at[0], gate_ref)
    load("up", up_hbm.at[0], up_ref)
    for t in range(4):
        load(("down", t), down_hbm.at[0, :, pl.ds(t * share, share)], down_ref.at[t])
    load("query_gain", query_gain_hbm, query_gain_ref)
    load("query", query_hbm, query_ref)
    load("w_query", w_query_hbm, w_query_ref)
    load("w_rope", w_rope_hbm, w_rope_ref)
    load("w_key", w_key_hbm, w_key_ref)
    load("w_value", w_value_hbm, w_value_ref)
    load("w_out", w_out_hbm, w_out_ref)

    def dot(left, right):
        return jnp.dot(left, right, preferred_element_type=jnp.float32)

    def dot_lanes(left, right):
        return lax.dot_general(
            left, right, (((1,), (1,)), ((), ())), preferred_element_type=jnp.float32
        )

    def wide(value):
        return value.astype(jnp.float32)

    def scaled(values_in, gain):
        widened = wide(values_in)
        mean = jnp.mean(widened * widened, axis=-1, keepdims=True)
        return (widened * lax.rsqrt(mean + epsilon) * gain).astype(jnp.bfloat16)

    def iota(shape, dim):
        return lax.broadcasted_iota(jnp.int32, shape, dim)

    def group_lines(group):
        return pl.ds(pl.multiple_of(group * rows, rows), rows)

    before = jnp.where(iota((tok_rows, tok_rows), 0) < iota((tok_rows, tok_rows), 1), 1.0, 0.0)
    before = before.astype(jnp.bfloat16)
    loads["route"].wait()
    first = route_ref[0:1, :]
    group = jnp.zeros_like(first)
    for g in range(1, GROUPS):
        group = group + (first >= g * TOPK).astype(jnp.int32)
    picks = jnp.broadcast_to(group, (8, tok_rows)) == iota((8, tok_rows), 0)
    picks = jnp.where(picks, 1.0, 0.0)
    earlier = dot(picks.astype(jnp.bfloat16), before)
    rank_of = jnp.sum(earlier * picks, axis=0, keepdims=True).astype(jnp.int32)
    place = group * rows + rank_of
    for g in range(GROUPS):
        hit = jnp.broadcast_to(place, (rows, tok_rows)) == iota((rows, tok_rows), 0) + g * rows
        order_ref[g * rows : (g + 1) * rows, :] = jnp.where(hit, 1.0, 0.0).astype(jnp.bfloat16)

    def split(value):
        top = value.astype(jnp.bfloat16)
        rest = value - wide(top)
        middle = rest.astype(jnp.bfloat16)
        return wide(top), wide(middle), rest - wide(middle)

    step_rows = 32

    def scale_step(step, unused):
        lines = pl.ds(pl.multiple_of(step * step_rows, step_rows), step_rows)
        widened = wide(tokens_ref[lines, :])
        mean = jnp.mean(widened * widened, axis=-1, keepdims=True)
        lane = iota((step_rows, 128), 1)
        table = jnp.zeros((step_rows, 128), jnp.float32)
        for k, value in enumerate(split(lax.rsqrt(mean + epsilon))):
            table = jnp.where(lane == k, jnp.broadcast_to(value, table.shape), table)
        scale_ref[lines, :] = table.astype(jnp.bfloat16)
        return unused

    per_load = tok_rows // 4 // step_rows
    for k in range(4):
        token_loads[k].wait()
        lax.fori_loop(k * per_load, (k + 1) * per_load, scale_step, 0, unroll=True)
    loads["gain"].wait()

    def remote(source, target, send, recv, peer):
        return pltpu.make_async_remote_copy(
            src_ref=source,
            dst_ref=target,
            send_sem=send,
            recv_sem=recv,
            device_id=peer,
            device_id_type=MESH,
        )

    def lines_at(u):
        return pl.ds(u % HALVES * lines_of, lines_of)

    def block_at(u):
        return flip(z, u // HALVES)

    def line_at(rel):
        return x if rel == 0 else 1 - x

    def z_copy(u):
        return remote(
            outgoing_ref.at[block_at(u), lines_at(u), carried(u)],
            member_ref.at[c, z, x, lines_at(u), carried(u)],
            z_send.at[u],
            z_recv.at[u],
            at_z(u // HALVES),
        )

    def w_copy(d):
        return remote(
            weight_ref.at[flip(z, d)], weight_in.at[z], w_send.at[d], w_recv.at[d], at_z(d)
        )

    def x_copy(u):
        piece = member_ref.at[c, block_at(u), x, lines_at(u), carried(u)]
        return remote(piece, piece, x_send.at[u], x_recv.at[u], at_x)

    def y_copy(u, rel):
        piece = member_ref.at[c, block_at(u), line_at(rel), lines_at(u), passed(u)]
        k = 2 * u + rel
        return remote(piece, piece, y_send.at[k], y_recv.at[k], at_y)

    def c_copy(u, rel):
        piece = member_ref.at[c, block_at(u), line_at(rel), lines_at(u)]
        k = 2 * u + rel
        return remote(piece, piece, c_send.at[k], c_recv.at[k], at_c)

    def p_copy(u):
        return remote(pair_send.at[u], pair_recv.at[u], p_send.at[u], p_recv.at[u], at_c)

    def x_leads(u):
        return u in X_LEADS

    def f_copy(u):
        peer = at_x if x_leads(u) else at_y
        return remote(first_send.at[u], first_recv.at[u], f_send.at[u], f_recv.at[u], peer)

    def s_copy(u):
        peer = at_y if x_leads(u) else at_x
        return remote(second_send.at[u], second_recv.at[u], s_send.at[u], s_recv.at[u], peer)

    def o_copy(u):
        return remote(
            fin_send.at[u],
            fin_ref.at[z, lines_at(u)],
            o_send.at[u],
            o_recv.at[u],
            at_z(u // HALVES),
        )

    def key_pair(view, send, recv, k, peer):
        return [
            remote(ref, ref, send.at[2 * k + i], recv.at[2 * k + i], peer)
            for i, ref in enumerate(view)
        ]

    def kz_copy(d):
        view = (keys_ref.at[z, x, c], turns_ref.at[z, x, c])
        return key_pair(view, kz_send, kz_recv, d, at_z(d))

    def kx_copy(d):
        view = (keys_ref.at[flip(z, d), x, c], turns_ref.at[flip(z, d), x, c])
        return key_pair(view, kx_send, kx_recv, d, at_x)

    def kc_copy(d):
        if d == 0:
            view = (keys_ref.at[z, 1 - x, c], turns_ref.at[z, 1 - x, c])
        else:
            view = (keys_ref.at[flip(z, d), :, c], turns_ref.at[flip(z, d), :, c])
        return key_pair(view, kc_send, kc_recv, d, at_c)

    def a_copy(yy):
        return remote(
            mixed_ref.at[yy * 2 + 1 - c], mixed_in.at[yy], a_send.at[yy], a_recv.at[yy], at_c
        )

    def j_copy():
        return remote(joint_send, joint_recv, j_send.at[0], j_recv.at[0], at_y)

    started = []

    def copies_of(maker, args):
        made = maker(*args)
        return made if isinstance(made, list) else [made]

    def start(maker, *args):
        for copy in copies_of(maker, args):
            copy.start()
        if (maker, args) not in started:
            started.append((maker, args))

    def arrive(maker, *args):
        for copy in copies_of(maker, args):
            copy.wait_recv()

    def scale_of(group_index):
        table = dot(order_ref[group_lines(group_index), :], scale_ref[...])
        return jnp.sum(table, axis=-1, keepdims=True)

    def permuted(group_index, scale, first_col, cols):
        place_of = pl.ds(pl.multiple_of(first_col, 128), cols)
        picked = dot(order_ref[group_lines(group_index), :], tokens_ref[:, place_of])
        return (picked * scale * gain_ref[:, place_of]).astype(jnp.bfloat16)

    def make_units(d):
        spare = min(spare_of(d * HALVES + h) for h in range(HALVES))
        kept = pl.ds(pl.multiple_of(y * spare, 128), half - spare)
        outgoing_ref[flip(z, d), :, kept] = permuted(
            flip(z, d), scale_of(flip(z, d)), c * half + y * spare, half - spare
        )

    def make_own():
        scale = scale_of(z)
        for part in range(2):
            member_ref[part, z, x] = permuted(z, scale, part * half, half)

    made = set()
    for u in SENDS:
        d = u // HALVES
        if d not in made:
            if d > 0:
                make_units(d)
            else:
                make_own()
            if not made:
                pl.semaphore_wait(barrier, 6)
            made.add(d)
        if d > 0:
            start(z_copy, u)
        else:
            start(x_copy, u)

    def send_weights():
        loads["share"].wait()
        first_is_even = picks_even(route_ref[0:1, :])
        even = jnp.where(first_is_even, share_ref[0:1, :], share_ref[1:2, :])
        odd = jnp.where(first_is_even, share_ref[1:2, :], share_ref[0:1, :])
        line = iota((8, tok_rows), 0)
        table = jnp.zeros((8, tok_rows), jnp.float32)
        for k, value in enumerate(split(even) + split(odd)):
            table = jnp.where(line == k, jnp.broadcast_to(value, table.shape), table)
        table = table.astype(jnp.bfloat16)
        for g in range(GROUPS):
            weight_ref[g] = dot_lanes(table, order_ref[g * rows : (g + 1) * rows, :])
        for d in (1, 3, 2):
            start(w_copy, d)

    def picks_even(chosen):
        odd = jnp.zeros(chosen.shape, jnp.bool_)
        for e in range(1, GROUPS * TOPK, TOPK):
            odd = odd | (chosen == e)
        return jnp.logical_not(odd)

    def set_columns(d):
        if d > 0:
            arrive(w_copy, d)
        tile = weight_ref[z] if d == 0 else weight_in[flip(z, d)]
        even = tile[0:1] + tile[1:2] + tile[2:3]
        odd = tile[3:4] + tile[4:5] + tile[5:6]
        for k, line in enumerate(
            (jnp.where(x == 0, even, odd), jnp.where(x == 0, odd, even))
        ):
            column_ref[d, k] = jnp.transpose(jnp.broadcast_to(line, (rows, rows)))

    attend_rows, rank = latent_ref.shape
    key_half = attend_rows // 2
    lanes = 2 * ROPE

    def tables():
        lane = iota((1, lanes), 1)
        pair = (lane & (ROPE - 1)) >> 1
        quarter = ROPE // 4
        inverse = jnp.zeros((1, lanes), jnp.float32)
        for j in range(quarter):
            rate = rotary_base ** (-2.0 * j / (ROPE // 2))
            inverse = jnp.where((pair & (quarter - 1)) == j, rate, inverse)
        position = (ep * attend_rows + iota((attend_rows, lanes), 0)).astype(jnp.float32)
        grid_row = jnp.floor(position * (1.0 / GRID_W))
        grid_col = position - grid_row * GRID_W
        angle = jnp.where(jnp.broadcast_to(pair, position.shape) < quarter, grid_row, grid_col)
        angle = angle * inverse
        return jnp.cos(angle), jnp.sin(angle)

    def swap_matrix():
        from_lane = iota((lanes, lanes), 0)
        to_lane = iota((lanes, lanes), 1)
        to_even = (to_lane & 1) == 0
        swap = jnp.where(to_even & (from_lane == to_lane + 1), -1.0, 0.0)
        swap = jnp.where(jnp.logical_not(to_even) & (from_lane == to_lane - 1), 1.0, swap)
        return swap.astype(jnp.bfloat16)

    def make_keys():
        cosine, sine = tables()
        swap = swap_matrix()
        low_lane = iota((key_half, lanes), 1) < ROPE
        for name in ("key_gain", "latent", "rope"):
            loads[name].wait()
        keys_ref[z, x] = scaled(latent_ref[...], key_gain_ref[...]).reshape(2, key_half, rank)
        twice = jnp.transpose(jnp.concatenate([wide(rope_ref[...])] * 2, axis=0))
        turned = twice * cosine + dot(twice.astype(jnp.bfloat16), swap) * sine
        packed = jnp.where(low_lane, turned[:key_half], turned[key_half:])
        turns_ref[z, x] = packed.astype(jnp.bfloat16).reshape(2, key_half // 2, lanes)
        start(kx_copy, 0)
        for d in (1, 3, 2):
            start(kz_copy, d)
        for name in ("query_gain", "query", "w_query", "w_rope"):
            loads[name].wait()
        query_normed = scaled(query_ref[...], query_gain_ref[...])
        query_nope_ref[...] = dot(query_normed, w_query_ref[...]).astype(jnp.bfloat16)
        swapped = dot(w_rope_ref[...], swap).astype(jnp.bfloat16)
        query_turn = dot(query_normed, w_rope_ref[...]) * cosine
        query_turn = query_turn + dot(query_normed, swapped) * sine
        low = iota((attend_rows, lanes), 1) < ROPE
        for head in range(2):
            own = jnp.where(low if head == 0 else jnp.logical_not(low), query_turn, 0.0)
            other = pltpu.roll(own, ROPE, 1)
            query_turn_ref[head, head] = own.astype(jnp.bfloat16)
            query_turn_ref[head, 1 - head] = other.astype(jnp.bfloat16)

    def make_back():
        for k in range(tok_rows // rows):
            spread = jnp.broadcast_to(wide(place[:, k * rows : (k + 1) * rows]), (rows, rows))
            spread = jnp.transpose(spread)
            for g in range(GROUPS):
                target = (iota((rows, rows), 1) + g * rows).astype(jnp.float32)
                hit = jnp.where(spread == target, 1.0, 0.0).astype(jnp.bfloat16)
                back_ref[g, k * rows : (k + 1) * rows, :] = hit

    def compute(u):
        low = member_ref[0, block_at(u), :, lines_at(u), :].reshape(2 * lines_of, half)
        high = member_ref[1, block_at(u), :, lines_at(u), :].reshape(2 * lines_of, half)

        def project(weights):
            return dot(low, weights[:half, :]) + dot(high, weights[half:, :])

        gate_act = project(gate_ref)
        up_act = project(up_ref)
        hidden = (gate_act / (1.0 + jnp.exp(-gate_act)) * up_act).astype(jnp.bfloat16)
        for yy in range(2):
            term = dot(hidden, down_ref[yy * 2 + 1 - c])
            pair_send[u, yy] = term.astype(jnp.bfloat16).reshape(2, lines_of, share)
        start(p_copy, u)
        for yy in range(2):
            term = dot(hidden, down_ref[yy * 2 + c])
            pair_keep[u, yy] = term.astype(jnp.bfloat16).reshape(2, lines_of, share)

    def weights_of(u):
        def columns(k):
            square = column_ref[u // HALVES, k, lines_at(u), :]
            return jnp.concatenate([square] * (share // rows), axis=1)

        return columns(0), columns(1)

    def attend():
        for name in ("w_key", "w_value", "w_out"):
            loads[name].wait()
        blocks = keys_ref.shape[0] * keys_ref.shape[1]
        latents = keys_ref[...].reshape(blocks * attend_rows, rank)
        turns = turns_ref[...].reshape(blocks * key_half, lanes)
        key_nope = dot(latents, w_key_ref[...]).astype(jnp.bfloat16)
        value_rows = dot(latents, w_value_ref[...]).astype(jnp.bfloat16)
        key_nope = key_nope.reshape(blocks, 2, key_half, key_nope.shape[1])
        value_rows = value_rows.reshape(blocks, 2, key_half, value_rows.shape[1])
        for head in range(w_query_ref.shape[1] // NOPE):
            own = slice(head * NOPE, (head + 1) * NOPE)
            scores = []
            for part in range(2):
                left = jnp.concatenate(
                    [query_nope_ref[:, own], query_turn_ref[head, part]], axis=1
                )
                keys = key_nope[:, part, :, own].reshape(blocks * key_half, NOPE)
                right = jnp.concatenate([keys, turns], axis=1)
                scores.append(dot_lanes(left, right) * (NOPE + ROPE) ** (-0.5))
            top = jnp.maximum(
                jnp.max(scores[0], axis=-1, keepdims=True),
                jnp.max(scores[1], axis=-1, keepdims=True),
            )
            totals = jnp.zeros(top.shape, jnp.float32)
            mixed = jnp.zeros((attend_rows, VDIM), jnp.float32)
            for part in range(2):
                raised = jnp.exp(scores[part] - top)
                totals = totals + jnp.sum(raised, axis=-1, keepdims=True)
                values = value_rows[:, part, :, own].reshape(blocks * key_half, VDIM)
                mixed = mixed + dot(raised.astype(jnp.bfloat16), values)
            heads_ref[:, own] = (mixed / totals).astype(jnp.bfloat16)
        for t in range(4):
            lines = slice(t * (attend_rows // 4), (t + 1) * (attend_rows // 4))
            mixed_ref[t] = dot(heads_ref[lines, :], w_out_ref[...]).astype(jnp.bfloat16)
        for yy in range(2):
            start(a_copy, yy)

    def attend_join():
        for yy in range(2):
            arrive(a_copy, yy)
        sums = wide(mixed_ref[(1 - y) * 2 + c]) + wide(mixed_in[1 - y])
        joint_send[...] = sums.astype(jnp.bfloat16)
        start(j_copy)

    def attend_last():
        arrive(j_copy)
        sums = wide(mixed_ref[y * 2 + c]) + wide(mixed_in[y]) + wide(joint_recv[...])
        mixer_ref[...] = sums.astype(jnp.bfloat16)

    def stage_first(u):
        arrive(p_copy, u)
        if x_leads(u):
            for yy in range(2):
                sums = wide(pair_keep[u, yy, 1 - x]) + wide(pair_recv[u, yy, 1 - x])
                first_send[u, yy] = sums.astype(jnp.bfloat16)
            start(f_copy, u)
            for yy in range(2):
                first_keep[u, yy] = wide(pair_keep[u, yy, x]) + wide(pair_recv[u, yy, x])
        else:
            for line in range(2):
                sums = wide(pair_keep[u, 1 - y, line]) + wide(pair_recv[u, 1 - y, line])
                first_send[u, line] = sums.astype(jnp.bfloat16)
            start(f_copy, u)
            for line in range(2):
                first_keep[u, line] = wide(pair_keep[u, y, line]) + wide(pair_recv[u, y, line])

    def stage_second(u):
        arrive(f_copy, u)
        if x_leads(u):
            mine, other = weights_of(u)
            sums = mine * first_keep[u, 1 - y] + other * wide(first_recv[u, 1 - y])
            second_send[u] = sums.astype(jnp.bfloat16)
            start(s_copy, u)
            second_keep[u] = mine * first_keep[u, y] + other * wide(first_recv[u, y])
        else:
            sums = first_keep[u, 1 - x] + wide(first_recv[u, 1 - x])
            second_send[u] = sums.astype(jnp.bfloat16)
            start(s_copy, u)
            sums = first_keep[u, x] + wide(first_recv[u, x])
            second_keep[u] = wide(sums.astype(jnp.bfloat16))

    def stage_last(u):
        arrive(s_copy, u)
        if x_leads(u):
            result = second_keep[u] + wide(second_recv[u])
        else:
            mine, other = weights_of(u)
            result = mine * second_keep[u] + other * wide(second_recv[u])
        if u // HALVES == 0:
            fin_ref[z, lines_at(u)] = result.astype(jnp.bfloat16)
        else:
            fin_send[u] = result.astype(jnp.bfloat16)
            start(o_copy, u)

    def from_z(u):
        arrive(z_copy, u)
        start(x_copy, u)
        start(y_copy, u, 0)

    def from_x(u):
        arrive(x_copy, u)
        start(y_copy, u, 1)

    def from_y(u, rel):
        arrive(y_copy, u, rel)
        start(c_copy, u, rel)

    def gathered(u):
        for rel in range(2):
            if u // HALVES > 0 or rel > 0:
                arrive(c_copy, u, rel)

    def wait_weights():
        for name in ("gate", "up"):
            loads[name].wait()
        for t in range(4):
            loads[("down", t)].wait()

    def from_kz(d):
        arrive(kz_copy, d)
        start(kx_copy, d)

    def from_kx(d):
        arrive(kx_copy, d)
        start(kc_copy, d)

    def from_kc(d):
        arrive(kc_copy, d)

    def back_term(d):
        return dot(back_ref[flip(z, d)], fin_ref[flip(z, d)])

    def returned(u):
        arrive(o_copy, u)

    def back_early():
        for d in (1, 3):
            for h in range(HALVES):
                returned(d * HALVES + h)
        moe_ref[...] = (back_term(0) + back_term(1) + back_term(3)).astype(jnp.bfloat16)

    def back_last():
        for h in range(HALVES):
            returned(2 * HALVES + h)
        moe_ref[...] = (wide(moe_ref[...]) + back_term(2)).astype(jnp.bfloat16)

    steps = {
        "z": from_z,
        "x": from_x,
        "y": from_y,
        "g": gathered,
        "m": compute,
        "1": stage_first,
        "2": stage_second,
        "3": stage_last,
        "weights": send_weights,
        "columns": set_columns,
        "keys": make_keys,
        "back": make_back,
        "loaded": wait_weights,
        "kz": from_kz,
        "kx": from_kx,
        "kc": from_kc,
        "attend": attend,
        "join": attend_join,
        "last": attend_last,
        "early": back_early,
        "final": back_last,
    }

    for item in SCHEDULE:
            where, text = "", item
            if item[0] in "<>":
                where, text = item[0], item[1:]
            name, *numbers = text.split(".")
            step = steps[name]
            values = [int(number) for number in numbers]
            if where == "":
                step(*values)
            else:
                pl.when(at_end if where == ">" else jnp.logical_not(at_end))(
                    functools.partial(step, *values)
                )
    for maker, args in started:
        for copy in copies_of(maker, args):
            copy.wait_send()


SCHEDULE = (
    "keys", "loaded", "<x.1", "z.2", "back", "x.0", "z.3", ">y.0.1", ">x.1", ">z.6", ">kz.1", "x.2",
    ">y.2.0", ">x.3", ">y.6.0", "z.7", "kx.0", ">y.1.1", "<z.6", "<y.2.0", "<y.0.1", "g.0", "m.0",
    ">kc.0", ">z.5", ">kx.1", "<x.3", "<y.1.1", "weights", "<kz.3", "<y.2.1", "<z.4", "<x.6",
    "<y.3.1", "<z.5", "<x.7", "<y.6.0", "<kz.1", "<y.3.0", "<y.4.0", "<y.6.1", "1.0", ">z.4", "g.1",
    "m.1", ">x.6", ">y.2.1", "<kz.2", "<x.5", "y.7.0", ">x.7", "g.2", "m.2", ">kz.2", ">y.3.0",
    ">x.5", ">y.5.0", ">y.3.1", "columns.2", "columns.1", ">y.6.1", ">y.4.0", ">kz.3", "<kc.0",
    "<kx.1", "<y.5.0", "<y.7.1", "1.1", "columns.0", "<x.4", "1.2", "g.3", "m.3", "g.6", "m.6",
    ">y.5.1", ">x.4", "1.3", "<kx.2", "<kc.1", "<kx.3", "<y.5.1", "1.6", ">y.7.1", ">kx.3", ">kx.2",
    ">kc.1", ">kc.2", "g.5", "m.5", ">y.4.1", "2.1", "2.2", "<kc.3", "<y.4.1", "g.7", "m.7", "1.5",
    "2.0", "2.3", "g.4", "m.4", ">kc.3", "2.6", "<kc.2", "3.1", "1.4", "columns.3", "1.7", "3.2",
    "attend", "2.5", "3.0", "3.6", "3.3", "join", "2.4", "2.7", "3.5", "3.4", "3.7", "last",
    "early", "final",
)


def expert_exchange(tokens_b, ffn_gain, route, share_of, w_gate, w_up, w_down, mixer_args):
    tok_rows, width = tokens_b.shape
    rows = tok_rows // GROUPS
    half = width // 2
    share = width // 4
    units = w_gate.shape[2]
    attend_rows, rank = mixer_args[1].shape
    head_cols = mixer_args[7].shape[1]
    rank_q = mixer_args[0].shape[1]
    count = GROUPS * HALVES
    part = rows // HALVES
    narrow, full = jnp.bfloat16, jnp.float32
    vmem = pl.BlockSpec(memory_space=pltpu.VMEM)
    anywhere = pl.BlockSpec(memory_space=pl.ANY)
    dma = pltpu.SemaphoreType.DMA
    operands = (
        tokens_b,
        ffn_gain.reshape(1, width),
        route,
        share_of,
        w_gate,
        w_up,
        w_down,
        *mixer_args,
    )
    return pl.pallas_call(
        expert_kernel,
        out_shape=(
            jax.ShapeDtypeStruct((tok_rows, share), narrow),
            jax.ShapeDtypeStruct((attend_rows // 4, width), narrow),
        ),
        in_specs=[anywhere] * len(operands),
        out_specs=(vmem, vmem),
        scratch_shapes=[
            pltpu.VMEM((tok_rows, width), narrow),
            pltpu.VMEM((1, width), full),
            pltpu.VMEM(route.shape, jnp.int32),
            pltpu.VMEM(share_of.shape, full),
            pltpu.VMEM((attend_rows, rank_q), narrow),
            pltpu.VMEM((attend_rows, rank), narrow),
            pltpu.VMEM((ROPE, attend_rows), narrow),
            pltpu.VMEM((1, rank_q), full),
            pltpu.VMEM((1, rank), full),
            pltpu.VMEM(mixer_args[5].shape, narrow),
            pltpu.VMEM(mixer_args[6].shape, narrow),
            pltpu.VMEM(mixer_args[7].shape, narrow),
            pltpu.VMEM(mixer_args[8].shape, narrow),
            pltpu.VMEM(mixer_args[9].shape, narrow),
            pltpu.VMEM((tok_rows, tok_rows), narrow),
            pltpu.VMEM((GROUPS, tok_rows, rows), narrow),
            pltpu.VMEM((GROUPS, 8, rows), full),
            pltpu.VMEM((GROUPS, 8, rows), full),
            pltpu.VMEM((GROUPS, 2, rows, rows), full),
            pltpu.VMEM((tok_rows, 128), narrow),
            pltpu.VMEM((GROUPS, rows, half), narrow),
            pltpu.VMEM((2, GROUPS, 2, rows, half), narrow),
            pltpu.VMEM((width, units), narrow),
            pltpu.VMEM((width, units), narrow),
            pltpu.VMEM((4, units, share), narrow),
            pltpu.VMEM((count, 2, 2, part, share), narrow),
            pltpu.VMEM((count, 2, 2, part, share), narrow),
            pltpu.VMEM((count, 2, 2, part, share), narrow),
            pltpu.VMEM((count, 2, part, share), narrow),
            pltpu.VMEM((count, 2, part, share), full),
            pltpu.VMEM((count, 2, part, share), narrow),
            pltpu.VMEM((count, part, share), narrow),
            pltpu.VMEM((count, part, share), full),
            pltpu.VMEM((count, part, share), narrow),
            pltpu.VMEM((count, part, share), narrow),
            pltpu.VMEM((GROUPS, rows, share), narrow),
            pltpu.VMEM((GROUPS, 2, 2, attend_rows // 2, rank), narrow),
            pltpu.VMEM((GROUPS, 2, 2, attend_rows // 4, 2 * ROPE), narrow),
            pltpu.VMEM((attend_rows, head_cols), narrow),
            pltpu.VMEM((2, 2, attend_rows, 2 * ROPE), narrow),
            pltpu.VMEM((attend_rows, head_cols), narrow),
            pltpu.VMEM((4, attend_rows // 4, width), narrow),
            pltpu.VMEM((2, attend_rows // 4, width), narrow),
            pltpu.VMEM((attend_rows // 4, width), narrow),
            pltpu.VMEM((attend_rows // 4, width), narrow),
            dma((4,)),
            dma((24,)),
        ]
        + [dma((count,))] * 4
        + [dma((2 * count,))] * 4
        + [dma((count,))] * 8
        + [dma((GROUPS,))] * 2
        + [dma((2 * GROUPS,))] * 6
        + [dma((2,))] * 4,
        compiler_params=pltpu.CompilerParams(
            collective_id=0, has_side_effects=True, vmem_limit_bytes=55 * 1024 * 1024
        ),
        cost_estimate=pl.CostEstimate(
            flops=40_000_000_000, bytes_accessed=8_000_000, transcendentals=0
        ),
        name="expert_exchange",
    )(*operands)


def paired(mixer, tokens_b, ffn_gain, route_expert, route_weight, w_gate, w_up, w_down):
    query_latent, key_latent, rope_key, query_gain, key_gain = mixer[:5]
    mixer_args = (
        query_latent,
        key_latent,
        rope_key.T,
        query_gain.reshape(1, -1),
        key_gain.reshape(1, -1),
        *mixer[5:],
    )
    moe_out, mixer_out = expert_exchange(
        tokens_b, ffn_gain, route_expert.T, route_weight.T, w_gate, w_up, w_down, mixer_args
    )
    return (mixer_out, moe_out)


def body(
    query_latent,
    key_latent,
    rope_key,
    query_gain,
    key_gain,
    w_query,
    w_query_rope,
    w_key,
    w_value,
    w_out,
    tokens_b,
    ffn_gain,
    route_expert,
    route_weight,
    w_gate,
    w_up,
    w_down,
):
    mixer = (
        query_latent,
        key_latent,
        rope_key,
        query_gain,
        key_gain,
        w_query,
        w_query_rope,
        w_key,
        w_value,
        w_out,
    )
    experts = (tokens_b, ffn_gain, route_expert, route_weight, w_gate, w_up, w_down)
    if (
        lax.axis_size("ep") == GROUPS * TOPK
        and lax.axis_size("tp") == 4
        and GROUPS == 4
        and tokens_b.shape[0] == GROUPS * 128
        and w_query.shape[1] == 2 * NOPE
    ):
        return paired(mixer, *experts)
    return (mixer_half(*mixer), expert_half(*experts))


def solution(mesh):
    in_specs = (
        P("ep", None),
        P("ep", None),
        P("ep", None),
        P(),
        P(),
        P(None, "tp"),
        P(None, "tp"),
        P(None, "tp"),
        P(None, "tp"),
        P("tp", None),
        P("ep", None),
        P(),
        P("ep", None),
        P("ep", None),
        P("ep", None, "tp"),
        P("ep", None, "tp"),
        P("ep", "tp", None),
    )
    out_specs = (P(("ep", "tp"), None), P("ep", "tp"))
    return jax.shard_map(body, mesh=mesh, in_specs=in_specs, out_specs=out_specs, check_vma=False)
```

```python
import functools
import math

import jax
import jax.numpy as jnp
from jax import lax
from jax.experimental import pallas as pl
from jax.experimental.pallas import tpu as pltpu
from jax.sharding import PartitionSpec as P

NOPE = 128
ROPE = 64
VDIM = 128
GRID_W = 64
TOPK = 2
GROUPS = 4
MESH = pl.DeviceIdType.MESH
HALVES = 2
Z_SPARES = (1, 1, 3, 2, 4, 4, 4, 4)
X_SPARES = (1, 1, 4, 2, 4, 4, 4, 4)
X_LEADS = (0, 1, 4, 6, 7)
SENDS = (2, 6, 3, 7, 0, 1, 4, 5)


epsilon = 1e-06
rotary_base = 10000.0
neg_large = -1e30


def rms_scale(values_in, gain):
    widened = values_in.astype(jnp.float32)
    normed = widened * lax.rsqrt(jnp.mean(widened * widened, axis=-1, keepdims=True) + epsilon)
    return (normed * gain).astype(jnp.bfloat16)


def rotary_tables(positions):
    half_width = ROPE // 2
    inverse = rotary_base ** (-jnp.arange(0, half_width, 2, dtype=jnp.float32) / half_width)
    grid_row = (positions // GRID_W).astype(jnp.float32)
    grid_col = (positions % GRID_W).astype(jnp.float32)
    angle = jnp.concatenate([grid_row[:, None] * inverse, grid_col[:, None] * inverse], axis=-1)
    return (jnp.cos(angle), jnp.sin(angle))


def rotate(values_in, cosine, sine):
    even_part = values_in[..., 0::2]
    odd_part = values_in[..., 1::2]
    turned = jnp.stack(
        [even_part * cosine - odd_part * sine, even_part * sine + odd_part * cosine], axis=-1
    )
    return turned.reshape(values_in.shape)


def fold_blocks(carry, members, step_fn):
    piece_rows = members[0].shape[0]
    block_rows = math.gcd(piece_rows, 1024)
    if block_rows == piece_rows:
        return step_fn(carry, members)
    stacked = tuple(
        (
            member.reshape((piece_rows // block_rows, block_rows) + member.shape[1:])
            for member in members
        )
    )

    def scan_step(inner_carry, blocks):
        return (step_fn(inner_carry, blocks), None)

    result, unused = lax.scan(scan_step, carry, stacked)
    return result


def mixer_half(
    query_latent,
    key_latent,
    rope_key,
    query_gain,
    key_gain,
    w_query,
    w_query_rope,
    w_key,
    w_value,
    w_out,
):
    tok_rows = query_latent.shape[0]
    local_heads = w_query.shape[1] // NOPE
    positions = lax.axis_index("ep") * tok_rows + jnp.arange(tok_rows, dtype=jnp.int32)
    cosine, sine = rotary_tables(positions)
    query_normed = rms_scale(query_latent, query_gain)
    query_nope = jnp.dot(query_normed, w_query, preferred_element_type=jnp.float32).astype(
        jnp.bfloat16
    )
    query_nope = query_nope.reshape(tok_rows, local_heads, NOPE)
    query_rot = jnp.dot(query_normed, w_query_rope, preferred_element_type=jnp.float32)
    query_rot = rotate(
        query_rot.reshape(tok_rows, local_heads, ROPE), cosine[:, None, :], sine[:, None, :]
    )
    query_rot = query_rot.astype(jnp.bfloat16)
    key_rot = rotate(rope_key.astype(jnp.float32), cosine, sine).astype(jnp.bfloat16)
    score_scale = (NOPE + ROPE) ** (-0.5)

    def expand(latent_rows):
        latent_count = latent_rows.shape[0]
        key_normed = rms_scale(latent_rows, key_gain)
        key_nope = jnp.dot(key_normed, w_key, preferred_element_type=jnp.float32).astype(
            jnp.bfloat16
        )
        value_rows = jnp.dot(key_normed, w_value, preferred_element_type=jnp.float32).astype(
            jnp.bfloat16
        )
        return (
            key_nope.reshape(latent_count, local_heads, NOPE),
            value_rows.reshape(latent_count, local_heads, VDIM),
        )

    def attend_block(carry, key_nope, value_rows, key_turn):
        run_max, run_total, run_acc = carry
        scores = jnp.einsum(
            "qhd,khd->hqk", query_nope, key_nope, preferred_element_type=jnp.float32
        )
        scores = scores + jnp.einsum(
            "qhd,kd->hqk", query_rot, key_turn, preferred_element_type=jnp.float32
        )
        scores = scores * score_scale
        new_max = jnp.maximum(run_max, jnp.max(scores, axis=-1))
        correction = jnp.exp(run_max - new_max)
        weights = jnp.exp(scores - new_max[..., None])
        new_total = run_total * correction + jnp.sum(weights, axis=-1)
        added = jnp.einsum(
            "hqk,khd->qhd",
            weights.astype(jnp.bfloat16),
            value_rows,
            preferred_element_type=jnp.float32,
        )
        new_acc = run_acc * jnp.transpose(correction)[..., None] + added
        return (new_max, new_total, new_acc)

    def step_latent(carry, blocks):
        key_nope, value_rows = expand(blocks[0])
        return attend_block(carry, key_nope, value_rows, blocks[1])

    initial = (
        jnp.full((local_heads, tok_rows), neg_large, jnp.float32),
        jnp.zeros((local_heads, tok_rows), jnp.float32),
        jnp.zeros((tok_rows, local_heads, VDIM), jnp.float32),
    )
    gathered = lax.all_gather(
        jnp.concatenate([key_latent, key_rot], axis=1), "ep", axis=0, tiled=True
    )
    rank = key_latent.shape[1]
    final = fold_blocks(initial, (gathered[:, :rank], gathered[:, rank:]), step_latent)
    run_max, run_total, run_acc = final
    heads_out = (run_acc / jnp.transpose(run_total)[..., None]).astype(jnp.bfloat16)
    heads_out = heads_out.reshape(tok_rows, local_heads * VDIM)
    return lax.psum_scatter(
        jnp.dot(heads_out, w_out, preferred_element_type=jnp.float32).astype(jnp.bfloat16),
        "tp",
        scatter_dimension=0,
        tiled=True,
    )


def expert_half(tokens_b, ffn_gain, route_expert, route_weight, w_gate, w_up, w_down):
    tok_rows = tokens_b.shape[0]
    expert_count = lax.axis_size("ep")
    capacity = TOPK * tok_rows // expert_count
    normed = rms_scale(tokens_b, ffn_gain)
    copies = route_expert.reshape(tok_rows * TOPK)
    chosen = (copies[:, None] == jnp.arange(expert_count, dtype=jnp.int32)[None, :]).astype(
        jnp.int32
    )
    earlier = jnp.cumsum(chosen, axis=0) - chosen
    slot_index = jnp.sum(earlier * chosen, axis=1)
    target = copies * capacity + slot_index
    source_row = (
        jnp.zeros((expert_count * capacity,), jnp.int32)
        .at[target]
        .set(jnp.arange(tok_rows * TOPK, dtype=jnp.int32) // TOPK)
    )
    outgoing = jnp.take(normed, source_row, axis=0)
    share_cols = outgoing.shape[1] // lax.axis_size("tp")
    own_cols = lax.dynamic_slice_in_dim(outgoing, lax.axis_index("tp") * share_cols, share_cols, 1)
    arrived = lax.all_to_all(own_cols, "ep", split_axis=0, concat_axis=0, tiled=True)
    member = lax.all_gather(arrived, "tp", axis=1, tiled=True)
    gate_rows = w_gate[0]
    up_rows = w_up[0]
    gate_act = jnp.dot(member, gate_rows, preferred_element_type=jnp.float32)
    up_act = jnp.dot(member, up_rows, preferred_element_type=jnp.float32)
    hidden = (jax.nn.silu(gate_act) * up_act).astype(jnp.bfloat16)
    partial_term = jnp.dot(hidden, w_down[0], preferred_element_type=jnp.float32)
    shared = lax.psum_scatter(
        partial_term.astype(jnp.bfloat16), "tp", scatter_dimension=1, tiled=True
    )
    returned = lax.all_to_all(shared, "ep", split_axis=0, concat_axis=0, tiled=True)
    picked = (
        jnp.take(returned, target, axis=0)
        .astype(jnp.float32)
        .reshape(tok_rows, TOPK, returned.shape[1])
    )
    combined = jnp.sum(picked * route_weight[:, :, None], axis=1)
    return combined.astype(jnp.bfloat16)


def flip(index, distance):
    low = index % 2
    high = index // 2
    if distance % 2 == 1:
        low = 1 - low
    if distance // 2 == 1:
        high = 1 - high
    return high * 2 + low


def expert_kernel(
    tokens_hbm,
    gain_hbm,
    route_hbm,
    weight_hbm,
    gate_hbm,
    up_hbm,
    down_hbm,
    query_hbm,
    latent_hbm,
    rope_hbm,
    query_gain_hbm,
    key_gain_hbm,
    w_query_hbm,
    w_rope_hbm,
    w_key_hbm,
    w_value_hbm,
    w_out_hbm,
    moe_ref,
    mixer_ref,
    tokens_ref,
    gain_ref,
    route_ref,
    share_ref,
    query_ref,
    latent_ref,
    rope_ref,
    query_gain_ref,
    key_gain_ref,
    w_query_ref,
    w_rope_ref,
    w_key_ref,
    w_value_ref,
    w_out_ref,
    order_ref,
    back_ref,
    weight_ref,
    weight_in,
    column_ref,
    scale_ref,
    outgoing_ref,
    member_ref,
    gate_ref,
    up_ref,
    down_ref,
    pair_send,
    pair_keep,
    pair_recv,
    first_send,
    first_keep,
    first_recv,
    second_send,
    second_keep,
    second_recv,
    fin_send,
    fin_ref,
    keys_ref,
    turns_ref,
    query_nope_ref,
    query_turn_ref,
    heads_ref,
    mixed_ref,
    mixed_in,
    joint_send,
    joint_recv,
    token_sem,
    load_sem,
    z_send,
    z_recv,
    x_send,
    x_recv,
    y_send,
    y_recv,
    c_send,
    c_recv,
    p_send,
    p_recv,
    f_send,
    f_recv,
    s_send,
    s_recv,
    o_send,
    o_recv,
    w_send,
    w_recv,
    kz_send,
    kz_recv,
    kx_send,
    kx_recv,
    kc_send,
    kc_recv,
    a_send,
    a_recv,
    j_send,
    j_recv,
):
    ep = lax.axis_index("ep")
    tp = lax.axis_index("tp")
    z, x = ep // 2, ep % 2
    y, c = tp // 2, tp % 2
    rows, half = outgoing_ref.shape[1:]
    lines_of = rows // HALVES
    tok_rows = tokens_ref.shape[0]
    share = fin_ref.shape[2]

    def sides(eighths):
        spare = half * eighths // 8
        kept = pl.ds(pl.multiple_of(y * spare, 128), half - spare)
        return kept, pl.ds(pl.multiple_of(y * (half - spare), 128), spare)

    def carried(u):
        return sides(Z_SPARES[u])[0]

    def forwarded(u):
        return sides(X_SPARES[u])[0]

    def passed(u, rel):
        return sides((Z_SPARES if rel == 0 else X_SPARES)[u])[1]

    at_end = (z == 0) | (z == GROUPS - 1)

    def at_z(distance):
        return {"ep": flip(z, distance) * 2 + x, "tp": tp}

    at_x = {"ep": z * 2 + 1 - x, "tp": tp}
    at_y = {"ep": ep, "tp": (1 - y) * 2 + c}
    at_c = {"ep": ep, "tp": y * 2 + 1 - c}

    barrier = pltpu.get_barrier_semaphore()
    for peer in (at_z(1), at_z(2), at_z(3), at_x, at_y, at_c):
        pl.semaphore_signal(barrier, inc=1, device_id=peer, device_id_type=MESH)

    loads = {}

    def load(name, source, target):
        loads[name] = pltpu.make_async_copy(source, target, load_sem.at[len(loads)])
        loads[name].start()

    load("route", route_hbm, route_ref)
    token_loads = []
    for k in range(4):
        lines = pl.ds(k * (tok_rows // 4), tok_rows // 4)
        token_loads.append(
            pltpu.make_async_copy(tokens_hbm.at[lines], tokens_ref.at[lines], token_sem.at[k])
        )
        token_loads[k].start()
    load("gain", gain_hbm, gain_ref)

    def load_rest():
        load("share", weight_hbm, share_ref)
        load("gate", gate_hbm.at[0], gate_ref)
        load("up", up_hbm.at[0], up_ref)
        for t in range(4):
            load(("down", t), down_hbm.at[0, :, pl.ds(t * share, share)], down_ref.at[t])
        load("key_gain", key_gain_hbm, key_gain_ref)
        load("latent", latent_hbm, latent_ref)
        load("rope", rope_hbm, rope_ref)
        load("query_gain", query_gain_hbm, query_gain_ref)
        load("query", query_hbm, query_ref)
        load("w_query", w_query_hbm, w_query_ref)
        load("w_rope", w_rope_hbm, w_rope_ref)
        load("w_key", w_key_hbm, w_key_ref)
        load("w_value", w_value_hbm, w_value_ref)
        load("w_out", w_out_hbm, w_out_ref)

    def dot(left, right):
        return jnp.dot(left, right, preferred_element_type=jnp.float32)

    def dot_lanes(left, right):
        return lax.dot_general(
            left, right, (((1,), (1,)), ((), ())), preferred_element_type=jnp.float32
        )

    def wide(value):
        return value.astype(jnp.float32)

    def scaled(values_in, gain):
        widened = wide(values_in)
        mean = jnp.mean(widened * widened, axis=-1, keepdims=True)
        return (widened * lax.rsqrt(mean + epsilon) * gain).astype(jnp.bfloat16)

    def iota(shape, dim):
        return lax.broadcasted_iota(jnp.int32, shape, dim)

    def group_lines(group):
        return pl.ds(pl.multiple_of(group * rows, rows), rows)

    before = jnp.where(iota((tok_rows, tok_rows), 0) < iota((tok_rows, tok_rows), 1), 1.0, 0.0)
    before = before.astype(jnp.bfloat16)
    loads["route"].wait()
    first = route_ref[0:1, :]
    group = jnp.zeros_like(first)
    for g in range(1, GROUPS):
        group = group + (first >= g * TOPK).astype(jnp.int32)
    picks = jnp.broadcast_to(group, (8, tok_rows)) == iota((8, tok_rows), 0)
    picks = jnp.where(picks, 1.0, 0.0)
    earlier = dot(picks.astype(jnp.bfloat16), before)
    rank_of = jnp.sum(earlier * picks, axis=0, keepdims=True).astype(jnp.int32)
    place = group * rows + rank_of
    for g in range(GROUPS):
        hit = jnp.broadcast_to(place, (rows, tok_rows)) == iota((rows, tok_rows), 0) + g * rows
        order_ref[g * rows : (g + 1) * rows, :] = jnp.where(hit, 1.0, 0.0).astype(jnp.bfloat16)

    def split(value):
        top = value.astype(jnp.bfloat16)
        rest = value - wide(top)
        middle = rest.astype(jnp.bfloat16)
        return wide(top), wide(middle), rest - wide(middle)

    width = tokens_ref.shape[1]
    for k in range(4):
        token_loads[k].wait()
        lines = slice(k * (tok_rows // 4), (k + 1) * (tok_rows // 4))
        squares = jnp.zeros((tok_rows // 4, 128), jnp.float32)
        for j in range(width // 128):
            widened = wide(tokens_ref[lines, j * 128 : (j + 1) * 128])
            squares = squares + widened * widened
        mean = jnp.sum(squares, axis=-1, keepdims=True) * (1.0 / width)
        lane = iota(squares.shape, 1)
        table = jnp.zeros(squares.shape, jnp.float32)
        for j, value in enumerate(split(lax.rsqrt(mean + epsilon))):
            table = jnp.where(lane == j, jnp.broadcast_to(value, table.shape), table)
        scale_ref[lines, :] = table.astype(jnp.bfloat16)
    loads["gain"].wait()
    load_rest()

    def remote(source, target, send, recv, peer):
        return pltpu.make_async_remote_copy(
            src_ref=source,
            dst_ref=target,
            send_sem=send,
            recv_sem=recv,
            device_id=peer,
            device_id_type=MESH,
        )

    def lines_at(u):
        return pl.ds(u % HALVES * lines_of, lines_of)

    def block_at(u):
        return flip(z, u // HALVES)

    def line_at(rel):
        return x if rel == 0 else 1 - x

    def z_copy(u):
        return remote(
            outgoing_ref.at[block_at(u), lines_at(u), carried(u)],
            member_ref.at[c, z, x, lines_at(u), carried(u)],
            z_send.at[u],
            z_recv.at[u],
            at_z(u // HALVES),
        )

    def w_copy(d):
        return remote(
            weight_ref.at[flip(z, d)], weight_in.at[z], w_send.at[d], w_recv.at[d], at_z(d)
        )

    def x_copy(u):
        piece = member_ref.at[c, block_at(u), x, lines_at(u), forwarded(u)]
        return remote(piece, piece, x_send.at[u], x_recv.at[u], at_x)

    def y_copy(u, rel):
        piece = member_ref.at[c, block_at(u), line_at(rel), lines_at(u), passed(u, rel)]
        k = 2 * u + rel
        return remote(piece, piece, y_send.at[k], y_recv.at[k], at_y)

    def c_copy(u, rel):
        piece = member_ref.at[c, block_at(u), line_at(rel), lines_at(u)]
        k = 2 * u + rel
        return remote(piece, piece, c_send.at[k], c_recv.at[k], at_c)

    def p_copy(u):
        return remote(pair_send.at[u], pair_recv.at[u], p_send.at[u], p_recv.at[u], at_c)

    def x_leads(u):
        return u in X_LEADS

    def f_copy(u):
        peer = at_x if x_leads(u) else at_y
        return remote(first_send.at[u], first_recv.at[u], f_send.at[u], f_recv.at[u], peer)

    def s_copy(u):
        peer = at_y if x_leads(u) else at_x
        return remote(second_send.at[u], second_recv.at[u], s_send.at[u], s_recv.at[u], peer)

    def o_copy(u):
        return remote(
            fin_send.at[u],
            fin_ref.at[z, lines_at(u)],
            o_send.at[u],
            o_recv.at[u],
            at_z(u // HALVES),
        )

    def key_pair(view, send, recv, k, peer):
        return [
            remote(ref, ref, send.at[2 * k + i], recv.at[2 * k + i], peer)
            for i, ref in enumerate(view)
        ]

    def kz_copy(d):
        view = (keys_ref.at[z, x, c], turns_ref.at[z, x, c])
        return key_pair(view, kz_send, kz_recv, d, at_z(d))

    def kx_copy(d):
        view = (keys_ref.at[flip(z, d), x, c], turns_ref.at[flip(z, d), x, c])
        return key_pair(view, kx_send, kx_recv, d, at_x)

    def kc_copy(d):
        if d == 0:
            view = (keys_ref.at[z, 1 - x, c], turns_ref.at[z, 1 - x, c])
        else:
            view = (keys_ref.at[flip(z, d), :, c], turns_ref.at[flip(z, d), :, c])
        return key_pair(view, kc_send, kc_recv, d, at_c)

    def a_copy(yy):
        return remote(
            mixed_ref.at[yy * 2 + 1 - c], mixed_in.at[yy], a_send.at[yy], a_recv.at[yy], at_c
        )

    def j_copy():
        return remote(joint_send, joint_recv, j_send.at[0], j_recv.at[0], at_y)

    started = []

    def copies_of(maker, args):
        made = maker(*args)
        return made if isinstance(made, list) else [made]

    def start(maker, *args):
        for copy in copies_of(maker, args):
            copy.start()
        if (maker, args) not in started:
            started.append((maker, args))

    def arrive(maker, *args):
        for copy in copies_of(maker, args):
            copy.wait_recv()

    def scale_of(group_index):
        table = dot(order_ref[group_lines(group_index), :], scale_ref[...])
        return jnp.sum(table, axis=-1, keepdims=True)

    def permuted(group_index, scale, first_col, cols):
        place_of = pl.ds(pl.multiple_of(first_col, 128), cols)
        picked = dot(order_ref[group_lines(group_index), :], tokens_ref[:, place_of])
        return (picked * scale * gain_ref[:, place_of]).astype(jnp.bfloat16)

    def make_units(d):
        eighths = min(Z_SPARES[d * HALVES + h] for h in range(HALVES))
        spare = half * eighths // 8
        outgoing_ref[flip(z, d), :, sides(eighths)[0]] = permuted(
            flip(z, d), scale_of(flip(z, d)), c * half + y * spare, half - spare
        )

    def make_own():
        scale = scale_of(z)
        for part in range(2):
            member_ref[part, z, x] = permuted(z, scale, part * half, half)

    made = set()
    for u in SENDS:
        d = u // HALVES
        if d not in made:
            if d > 0:
                make_units(d)
            else:
                make_own()
            if not made:
                pl.semaphore_wait(barrier, 6)
            made.add(d)
        if d > 0:
            start(z_copy, u)
        else:
            start(x_copy, u)

    def send_weights():
        loads["share"].wait()
        first_is_even = picks_even(route_ref[0:1, :])
        even = jnp.where(first_is_even, share_ref[0:1, :], share_ref[1:2, :])
        odd = jnp.where(first_is_even, share_ref[1:2, :], share_ref[0:1, :])
        line = iota((8, tok_rows), 0)
        table = jnp.zeros((8, tok_rows), jnp.float32)
        for k, value in enumerate(split(even) + split(odd)):
            table = jnp.where(line == k, jnp.broadcast_to(value, table.shape), table)
        table = table.astype(jnp.bfloat16)
        for g in range(GROUPS):
            weight_ref[g] = dot_lanes(table, order_ref[g * rows : (g + 1) * rows, :])
        for d in (1, 3, 2):
            start(w_copy, d)

    def picks_even(chosen):
        odd = jnp.zeros(chosen.shape, jnp.bool_)
        for e in range(1, GROUPS * TOPK, TOPK):
            odd = odd | (chosen == e)
        return jnp.logical_not(odd)

    def set_columns(d):
        if d > 0:
            arrive(w_copy, d)
        tile = weight_ref[z] if d == 0 else weight_in[flip(z, d)]
        even = tile[0:1] + tile[1:2] + tile[2:3]
        odd = tile[3:4] + tile[4:5] + tile[5:6]
        for k, line in enumerate(
            (jnp.where(x == 0, even, odd), jnp.where(x == 0, odd, even))
        ):
            column_ref[d, k] = jnp.transpose(jnp.broadcast_to(line, (rows, rows)))

    attend_rows, rank = latent_ref.shape
    key_half = attend_rows // 2
    lanes = 2 * ROPE

    def tables():
        lane = iota((1, lanes), 1)
        pair = (lane & (ROPE - 1)) >> 1
        quarter = ROPE // 4
        inverse = jnp.zeros((1, lanes), jnp.float32)
        for j in range(quarter):
            rate = rotary_base ** (-2.0 * j / (ROPE // 2))
            inverse = jnp.where((pair & (quarter - 1)) == j, rate, inverse)
        position = (ep * attend_rows + iota((attend_rows, lanes), 0)).astype(jnp.float32)
        grid_row = jnp.floor(position * (1.0 / GRID_W))
        grid_col = position - grid_row * GRID_W
        angle = jnp.where(jnp.broadcast_to(pair, position.shape) < quarter, grid_row, grid_col)
        angle = angle * inverse
        return jnp.cos(angle), jnp.sin(angle)

    def swap_matrix():
        from_lane = iota((lanes, lanes), 0)
        to_lane = iota((lanes, lanes), 1)
        to_even = (to_lane & 1) == 0
        swap = jnp.where(to_even & (from_lane == to_lane + 1), -1.0, 0.0)
        swap = jnp.where(jnp.logical_not(to_even) & (from_lane == to_lane - 1), 1.0, swap)
        return swap.astype(jnp.bfloat16)

    def make_keys():
        cosine, sine = tables()
        swap = swap_matrix()
        low_lane = iota((key_half, lanes), 1) < ROPE
        for name in ("key_gain", "latent", "rope"):
            loads[name].wait()
        keys_ref[z, x] = scaled(latent_ref[...], key_gain_ref[...]).reshape(2, key_half, rank)
        twice = jnp.transpose(jnp.concatenate([wide(rope_ref[...])] * 2, axis=0))
        turned = twice * cosine + dot(twice.astype(jnp.bfloat16), swap) * sine
        packed = jnp.where(low_lane, turned[:key_half], turned[key_half:])
        turns_ref[z, x] = packed.astype(jnp.bfloat16).reshape(2, key_half // 2, lanes)
        start(kx_copy, 0)
        for d in (1, 3, 2):
            start(kz_copy, d)
        for name in ("query_gain", "query", "w_query", "w_rope"):
            loads[name].wait()
        query_normed = scaled(query_ref[...], query_gain_ref[...])
        query_nope_ref[...] = dot(query_normed, w_query_ref[...]).astype(jnp.bfloat16)
        swapped = dot(w_rope_ref[...], swap).astype(jnp.bfloat16)
        query_turn = dot(query_normed, w_rope_ref[...]) * cosine
        query_turn = query_turn + dot(query_normed, swapped) * sine
        low = iota((attend_rows, lanes), 1) < ROPE
        for head in range(2):
            own = jnp.where(low if head == 0 else jnp.logical_not(low), query_turn, 0.0)
            other = pltpu.roll(own, ROPE, 1)
            query_turn_ref[head, head] = own.astype(jnp.bfloat16)
            query_turn_ref[head, 1 - head] = other.astype(jnp.bfloat16)

    def make_back():
        for k in range(tok_rows // rows):
            spread = jnp.broadcast_to(wide(place[:, k * rows : (k + 1) * rows]), (rows, rows))
            spread = jnp.transpose(spread)
            for g in range(GROUPS):
                target = (iota((rows, rows), 1) + g * rows).astype(jnp.float32)
                hit = jnp.where(spread == target, 1.0, 0.0).astype(jnp.bfloat16)
                back_ref[g, k * rows : (k + 1) * rows, :] = hit

    def compute(u):
        low = member_ref[0, block_at(u), :, lines_at(u), :].reshape(2 * lines_of, half)
        high = member_ref[1, block_at(u), :, lines_at(u), :].reshape(2 * lines_of, half)

        def project(weights):
            return dot(low, weights[:half, :]) + dot(high, weights[half:, :])

        gate_act = project(gate_ref)
        up_act = project(up_ref)
        hidden = (gate_act / (1.0 + jnp.exp(-gate_act)) * up_act).astype(jnp.bfloat16)
        for yy in range(2):
            term = dot(hidden, down_ref[yy * 2 + 1 - c])
            pair_send[u, yy] = term.astype(jnp.bfloat16).reshape(2, lines_of, share)
        start(p_copy, u)
        for yy in range(2):
            term = dot(hidden, down_ref[yy * 2 + c])
            pair_keep[u, yy] = term.astype(jnp.bfloat16).reshape(2, lines_of, share)

    def weights_of(u):
        def columns(k):
            square = column_ref[u // HALVES, k, lines_at(u), :]
            return jnp.concatenate([square] * (share // rows), axis=1)

        return columns(0), columns(1)

    def attend():
        for name in ("w_key", "w_value", "w_out"):
            loads[name].wait()
        blocks = keys_ref.shape[0] * keys_ref.shape[1]
        latents = keys_ref[...].reshape(blocks * attend_rows, rank)
        turns = turns_ref[...].reshape(blocks * key_half, lanes)
        key_nope = dot(latents, w_key_ref[...]).astype(jnp.bfloat16)
        value_rows = dot(latents, w_value_ref[...]).astype(jnp.bfloat16)
        key_nope = key_nope.reshape(blocks, 2, key_half, key_nope.shape[1])
        value_rows = value_rows.reshape(blocks, 2, key_half, value_rows.shape[1])
        for head in range(w_query_ref.shape[1] // NOPE):
            own = slice(head * NOPE, (head + 1) * NOPE)
            scores = []
            for part in range(2):
                left = jnp.concatenate(
                    [query_nope_ref[:, own], query_turn_ref[head, part]], axis=1
                )
                keys = key_nope[:, part, :, own].reshape(blocks * key_half, NOPE)
                right = jnp.concatenate([keys, turns], axis=1)
                scores.append(dot_lanes(left, right) * (NOPE + ROPE) ** (-0.5))
            top = jnp.maximum(
                jnp.max(scores[0], axis=-1, keepdims=True),
                jnp.max(scores[1], axis=-1, keepdims=True),
            )
            totals = jnp.zeros(top.shape, jnp.float32)
            mixed = jnp.zeros((attend_rows, VDIM), jnp.float32)
            for part in range(2):
                raised = jnp.exp(scores[part] - top)
                totals = totals + jnp.sum(raised, axis=-1, keepdims=True)
                values = value_rows[:, part, :, own].reshape(blocks * key_half, VDIM)
                mixed = mixed + dot(raised.astype(jnp.bfloat16), values)
            heads_ref[:, own] = (mixed / totals).astype(jnp.bfloat16)
        for t in range(4):
            lines = slice(t * (attend_rows // 4), (t + 1) * (attend_rows // 4))
            mixed_ref[t] = dot(heads_ref[lines, :], w_out_ref[...]).astype(jnp.bfloat16)
        for yy in range(2):
            start(a_copy, yy)

    def attend_join():
        for yy in range(2):
            arrive(a_copy, yy)
        sums = wide(mixed_ref[(1 - y) * 2 + c]) + wide(mixed_in[1 - y])
        joint_send[...] = sums.astype(jnp.bfloat16)
        start(j_copy)

    def attend_last():
        arrive(j_copy)
        sums = wide(mixed_ref[y * 2 + c]) + wide(mixed_in[y]) + wide(joint_recv[...])
        mixer_ref[...] = sums.astype(jnp.bfloat16)

    def stage_first(u):
        arrive(p_copy, u)
        if x_leads(u):
            for yy in range(2):
                sums = wide(pair_keep[u, yy, 1 - x]) + wide(pair_recv[u, yy, 1 - x])
                first_send[u, yy] = sums.astype(jnp.bfloat16)
            start(f_copy, u)
            for yy in range(2):
                first_keep[u, yy] = wide(pair_keep[u, yy, x]) + wide(pair_recv[u, yy, x])
        else:
            for line in range(2):
                sums = wide(pair_keep[u, 1 - y, line]) + wide(pair_recv[u, 1 - y, line])
                first_send[u, line] = sums.astype(jnp.bfloat16)
            start(f_copy, u)
            for line in range(2):
                first_keep[u, line] = wide(pair_keep[u, y, line]) + wide(pair_recv[u, y, line])

    def stage_second(u):
        arrive(f_copy, u)
        if x_leads(u):
            mine, other = weights_of(u)
            sums = mine * first_keep[u, 1 - y] + other * wide(first_recv[u, 1 - y])
            second_send[u] = sums.astype(jnp.bfloat16)
            start(s_copy, u)
            second_keep[u] = mine * first_keep[u, y] + other * wide(first_recv[u, y])
        else:
            sums = first_keep[u, 1 - x] + wide(first_recv[u, 1 - x])
            second_send[u] = sums.astype(jnp.bfloat16)
            start(s_copy, u)
            sums = first_keep[u, x] + wide(first_recv[u, x])
            second_keep[u] = wide(sums.astype(jnp.bfloat16))

    def stage_last(u):
        arrive(s_copy, u)
        if x_leads(u):
            result = second_keep[u] + wide(second_recv[u])
        else:
            mine, other = weights_of(u)
            result = mine * second_keep[u] + other * wide(second_recv[u])
        if u // HALVES == 0:
            fin_ref[z, lines_at(u)] = result.astype(jnp.bfloat16)
        else:
            fin_send[u] = result.astype(jnp.bfloat16)
            start(o_copy, u)

    def from_z(u):
        arrive(z_copy, u)
        start(x_copy, u)
        if Z_SPARES[u] > 0:
            start(y_copy, u, 0)

    def from_x(u):
        arrive(x_copy, u)
        start(y_copy, u, 1)

    def from_y(u, rel):
        if rel == 1 or Z_SPARES[u] > 0:
            arrive(y_copy, u, rel)
        start(c_copy, u, rel)

    def gathered(u):
        for rel in range(2):
            if u // HALVES > 0 or rel > 0:
                arrive(c_copy, u, rel)

    def wait_weights():
        for name in ("gate", "up"):
            loads[name].wait()
        for t in range(4):
            loads[("down", t)].wait()

    def from_kz(d):
        arrive(kz_copy, d)
        start(kx_copy, d)

    def from_kx(d):
        arrive(kx_copy, d)
        start(kc_copy, d)

    def from_kc(d):
        arrive(kc_copy, d)

    added = []

    def give_back(d):
        if d > 0:
            for h in range(HALVES):
                arrive(o_copy, d * HALVES + h)
        term = dot(back_ref[flip(z, d)], fin_ref[flip(z, d)])
        if added:
            term = term + wide(moe_ref[...])
        added.append(d)
        moe_ref[...] = term.astype(jnp.bfloat16)

    steps = {
        "z": from_z,
        "x": from_x,
        "y": from_y,
        "g": gathered,
        "m": compute,
        "1": stage_first,
        "2": stage_second,
        "3": stage_last,
        "weights": send_weights,
        "columns": set_columns,
        "keys": make_keys,
        "back": make_back,
        "loaded": wait_weights,
        "kz": from_kz,
        "kx": from_kx,
        "kc": from_kc,
        "attend": attend,
        "join": attend_join,
        "last": attend_last,
        "b": give_back,
    }

    for item in SCHEDULE:
            where, text = "", item
            if item[0] in "<>":
                where, text = item[0], item[1:]
            name, *numbers = text.split(".")
            step = steps[name]
            values = [int(number) for number in numbers]
            if where == "":
                step(*values)
            else:
                pl.when(at_end if where == ">" else jnp.logical_not(at_end))(
                    functools.partial(step, *values)
                )
    for maker, args in started:
        for copy in copies_of(maker, args):
            copy.wait_send()


SCHEDULE = (
    "z.2", "<z.7", "x.0", "<z.6", "<x.1", "<y.2.0", "z.3", "<y.1.1", "y.0.1", ">x.1", ">z.6",
    ">x.2", "keys", "<x.6", "<x.2", "z.4", "<kz.1", "loaded", ">y.1.1", ">z.7", "g.0", "m.0",
    "<z.5", "<y.6.1", "weights", ">z.5", ">y.2.1", "g.1", "m.1", ">x.6", ">kz.1", ">y.2.0", "<x.3",
    "<x.4", "<y.2.1", "<kz.3", "<kz.2", "1.0", ">x.3", "<y.5.0", "<y.6.0", "<x.7", "<y.7.0",
    "<y.4.0", "g.2", "m.2", ">y.3.0", ">y.6.0", "x.5", ">y.4.0", ">y.6.1", ">x.4", ">kz.2", "1.2",
    ">y.5.0", ">kz.3", ">y.7.0", ">kx.0", "<y.4.1", "<kx.2", "y.3.1", "columns.0", "1.1", "g.6",
    "m.6", ">kx.2", "2.0", "columns.2", "y.5.1", ">x.7", ">y.4.1", "1.6", "g.5", "m.5", "<y.3.0",
    "g.4", "m.4", "<y.7.1", "2.2", "<kc.2", "<kx.0", "<kx.3", "columns.3", "1.5", ">kx.1", "g.3",
    "m.3", ">kc.2", "3.0", "1.4", "<kc.0", "back", ">kc.0", ">y.7.1", "2.6", "1.3", "g.7", "m.7",
    ">kc.1", ">kx.3", "columns.1", "<kx.1", "2.5", "3.2", "<kc.3", "1.7", "2.1", "3.6", "2.4",
    "<kc.1", "3.5", ">kc.3", "attend", "3.1", "3.4", "2.7", "2.3", "join", "3.7", "3.3", "b.2",
    "b.0", "last", "b.1", "b.3",
)


def expert_exchange(tokens_b, ffn_gain, route, share_of, w_gate, w_up, w_down, mixer_args):
    tok_rows, width = tokens_b.shape
    rows = tok_rows // GROUPS
    half = width // 2
    share = width // 4
    units = w_gate.shape[2]
    attend_rows, rank = mixer_args[1].shape
    head_cols = mixer_args[7].shape[1]
    rank_q = mixer_args[0].shape[1]
    count = GROUPS * HALVES
    part = rows // HALVES
    narrow, full = jnp.bfloat16, jnp.float32
    vmem = pl.BlockSpec(memory_space=pltpu.VMEM)
    anywhere = pl.BlockSpec(memory_space=pl.ANY)
    dma = pltpu.SemaphoreType.DMA
    operands = (
        tokens_b,
        ffn_gain.reshape(1, width),
        route,
        share_of,
        w_gate,
        w_up,
        w_down,
        *mixer_args,
    )
    return pl.pallas_call(
        expert_kernel,
        out_shape=(
            pltpu.VMEM((tok_rows, share), narrow),
            pltpu.VMEM((attend_rows // 4, width), narrow),
        ),
        in_specs=[anywhere] * len(operands),
        out_specs=(vmem, vmem),
        scratch_shapes=[
            pltpu.VMEM((tok_rows, width), narrow),
            pltpu.VMEM((1, width), full),
            pltpu.VMEM(route.shape, jnp.int32),
            pltpu.VMEM(share_of.shape, full),
            pltpu.VMEM((attend_rows, rank_q), narrow),
            pltpu.VMEM((attend_rows, rank), narrow),
            pltpu.VMEM((ROPE, attend_rows), narrow),
            pltpu.VMEM((1, rank_q), full),
            pltpu.VMEM((1, rank), full),
            pltpu.VMEM(mixer_args[5].shape, narrow),
            pltpu.VMEM(mixer_args[6].shape, narrow),
            pltpu.VMEM(mixer_args[7].shape, narrow),
            pltpu.VMEM(mixer_args[8].shape, narrow),
            pltpu.VMEM(mixer_args[9].shape, narrow),
            pltpu.VMEM((tok_rows, tok_rows), narrow),
            pltpu.VMEM((GROUPS, tok_rows, rows), narrow),
            pltpu.VMEM((GROUPS, 8, rows), full),
            pltpu.VMEM((GROUPS, 8, rows), full),
            pltpu.VMEM((GROUPS, 2, rows, rows), full),
            pltpu.VMEM((tok_rows, 128), narrow),
            pltpu.VMEM((GROUPS, rows, half), narrow),
            pltpu.VMEM((2, GROUPS, 2, rows, half), narrow),
            pltpu.VMEM((width, units), narrow),
            pltpu.VMEM((width, units), narrow),
            pltpu.VMEM((4, units, share), narrow),
            pltpu.VMEM((count, 2, 2, part, share), narrow),
            pltpu.VMEM((count, 2, 2, part, share), narrow),
            pltpu.VMEM((count, 2, 2, part, share), narrow),
            pltpu.VMEM((count, 2, part, share), narrow),
            pltpu.VMEM((count, 2, part, share), full),
            pltpu.VMEM((count, 2, part, share), narrow),
            pltpu.VMEM((count, part, share), narrow),
            pltpu.VMEM((count, part, share), full),
            pltpu.VMEM((count, part, share), narrow),
            pltpu.VMEM((count, part, share), narrow),
            pltpu.VMEM((GROUPS, rows, share), narrow),
            pltpu.VMEM((GROUPS, 2, 2, attend_rows // 2, rank), narrow),
            pltpu.VMEM((GROUPS, 2, 2, attend_rows // 4, 2 * ROPE), narrow),
            pltpu.VMEM((attend_rows, head_cols), narrow),
            pltpu.VMEM((2, 2, attend_rows, 2 * ROPE), narrow),
            pltpu.VMEM((attend_rows, head_cols), narrow),
            pltpu.VMEM((4, attend_rows // 4, width), narrow),
            pltpu.VMEM((2, attend_rows // 4, width), narrow),
            pltpu.VMEM((attend_rows // 4, width), narrow),
            pltpu.VMEM((attend_rows // 4, width), narrow),
            dma((4,)),
            dma((24,)),
        ]
        + [dma((count,))] * 4
        + [dma((2 * count,))] * 4
        + [dma((count,))] * 8
        + [dma((GROUPS,))] * 2
        + [dma((2 * GROUPS,))] * 6
        + [dma((2,))] * 4,
        compiler_params=pltpu.CompilerParams(
            collective_id=0, has_side_effects=True, vmem_limit_bytes=48 * 1024 * 1024
        ),
        cost_estimate=pl.CostEstimate(
            flops=40_000_000_000, bytes_accessed=8_000_000, transcendentals=0
        ),
        name="expert_exchange",
    )(*(pltpu.with_memory_space_constraint(operand, pltpu.HBM) for operand in operands))


def paired(mixer, tokens_b, ffn_gain, route_expert, route_weight, w_gate, w_up, w_down):
    query_latent, key_latent, rope_key, query_gain, key_gain = mixer[:5]
    mixer_args = (
        query_latent,
        key_latent,
        rope_key.T,
        query_gain.reshape(1, -1),
        key_gain.reshape(1, -1),
        *mixer[5:],
    )
    moe_out, mixer_out = expert_exchange(
        tokens_b, ffn_gain, route_expert.T, route_weight.T, w_gate, w_up, w_down, mixer_args
    )
    return (mixer_out, moe_out)


def body(
    query_latent,
    key_latent,
    rope_key,
    query_gain,
    key_gain,
    w_query,
    w_query_rope,
    w_key,
    w_value,
    w_out,
    tokens_b,
    ffn_gain,
    route_expert,
    route_weight,
    w_gate,
    w_up,
    w_down,
):
    mixer = (
        query_latent,
        key_latent,
        rope_key,
        query_gain,
        key_gain,
        w_query,
        w_query_rope,
        w_key,
        w_value,
        w_out,
    )
    experts = (tokens_b, ffn_gain, route_expert, route_weight, w_gate, w_up, w_down)
    if (
        lax.axis_size("ep") == GROUPS * TOPK
        and lax.axis_size("tp") == 4
        and GROUPS == 4
        and tokens_b.shape[0] == GROUPS * 128
        and w_query.shape[1] == 2 * NOPE
    ):
        return paired(mixer, *experts)
    return (mixer_half(*mixer), expert_half(*experts))


def solution(mesh):
    in_specs = (
        P("ep", None),
        P("ep", None),
        P("ep", None),
        P(),
        P(),
        P(None, "tp"),
        P(None, "tp"),
        P(None, "tp"),
        P(None, "tp"),
        P("tp", None),
        P("ep", None),
        P(),
        P("ep", None),
        P("ep", None),
        P("ep", None, "tp"),
        P("ep", None, "tp"),
        P("ep", "tp", None),
    )
    out_specs = (P(("ep", "tp"), None), P("ep", "tp"))
    return jax.shard_map(body, mesh=mesh, in_specs=in_specs, out_specs=out_specs, check_vma=False)
```

```python
import functools
import math

import jax
import jax.numpy as jnp
from jax import lax
from jax.experimental import pallas as pl
from jax.experimental.pallas import tpu as pltpu
from jax.sharding import PartitionSpec as P

NOPE = 128
ROPE = 64
VDIM = 128
GRID_W = 64
TOPK = 2
GROUPS = 4
MESH = pl.DeviceIdType.MESH
HALVES = 2
Z_SPARES = (3, 3, 3, 3, 4, 3, 4, 4)
X_SPARES = (3, 3, 3, 3, 4, 3, 4, 4)
X_LEADS = (1, 4, 5, 6, 7)
SENDS = (2, 6, 3, 0, 1, 7, 4, 5)


epsilon = 1e-06
rotary_base = 10000.0
neg_large = -1e30


def rms_scale(values_in, gain):
    widened = values_in.astype(jnp.float32)
    normed = widened * lax.rsqrt(jnp.mean(widened * widened, axis=-1, keepdims=True) + epsilon)
    return (normed * gain).astype(jnp.bfloat16)


def rotary_tables(positions):
    half_width = ROPE // 2
    inverse = rotary_base ** (-jnp.arange(0, half_width, 2, dtype=jnp.float32) / half_width)
    grid_row = (positions // GRID_W).astype(jnp.float32)
    grid_col = (positions % GRID_W).astype(jnp.float32)
    angle = jnp.concatenate([grid_row[:, None] * inverse, grid_col[:, None] * inverse], axis=-1)
    return (jnp.cos(angle), jnp.sin(angle))


def rotate(values_in, cosine, sine):
    even_part = values_in[..., 0::2]
    odd_part = values_in[..., 1::2]
    turned = jnp.stack(
        [even_part * cosine - odd_part * sine, even_part * sine + odd_part * cosine], axis=-1
    )
    return turned.reshape(values_in.shape)


def fold_blocks(carry, members, step_fn):
    piece_rows = members[0].shape[0]
    block_rows = math.gcd(piece_rows, 1024)
    if block_rows == piece_rows:
        return step_fn(carry, members)
    stacked = tuple(
        (
            member.reshape((piece_rows // block_rows, block_rows) + member.shape[1:])
            for member in members
        )
    )

    def scan_step(inner_carry, blocks):
        return (step_fn(inner_carry, blocks), None)

    result, unused = lax.scan(scan_step, carry, stacked)
    return result


def mixer_half(
    query_latent,
    key_latent,
    rope_key,
    query_gain,
    key_gain,
    w_query,
    w_query_rope,
    w_key,
    w_value,
    w_out,
):
    tok_rows = query_latent.shape[0]
    local_heads = w_query.shape[1] // NOPE
    positions = lax.axis_index("ep") * tok_rows + jnp.arange(tok_rows, dtype=jnp.int32)
    cosine, sine = rotary_tables(positions)
    query_normed = rms_scale(query_latent, query_gain)
    query_nope = jnp.dot(query_normed, w_query, preferred_element_type=jnp.float32).astype(
        jnp.bfloat16
    )
    query_nope = query_nope.reshape(tok_rows, local_heads, NOPE)
    query_rot = jnp.dot(query_normed, w_query_rope, preferred_element_type=jnp.float32)
    query_rot = rotate(
        query_rot.reshape(tok_rows, local_heads, ROPE), cosine[:, None, :], sine[:, None, :]
    )
    query_rot = query_rot.astype(jnp.bfloat16)
    key_rot = rotate(rope_key.astype(jnp.float32), cosine, sine).astype(jnp.bfloat16)
    score_scale = (NOPE + ROPE) ** (-0.5)

    def expand(latent_rows):
        latent_count = latent_rows.shape[0]
        key_normed = rms_scale(latent_rows, key_gain)
        key_nope = jnp.dot(key_normed, w_key, preferred_element_type=jnp.float32).astype(
            jnp.bfloat16
        )
        value_rows = jnp.dot(key_normed, w_value, preferred_element_type=jnp.float32).astype(
            jnp.bfloat16
        )
        return (
            key_nope.reshape(latent_count, local_heads, NOPE),
            value_rows.reshape(latent_count, local_heads, VDIM),
        )

    def attend_block(carry, key_nope, value_rows, key_turn):
        run_max, run_total, run_acc = carry
        scores = jnp.einsum(
            "qhd,khd->hqk", query_nope, key_nope, preferred_element_type=jnp.float32
        )
        scores = scores + jnp.einsum(
            "qhd,kd->hqk", query_rot, key_turn, preferred_element_type=jnp.float32
        )
        scores = scores * score_scale
        new_max = jnp.maximum(run_max, jnp.max(scores, axis=-1))
        correction = jnp.exp(run_max - new_max)
        weights = jnp.exp(scores - new_max[..., None])
        new_total = run_total * correction + jnp.sum(weights, axis=-1)
        added = jnp.einsum(
            "hqk,khd->qhd",
            weights.astype(jnp.bfloat16),
            value_rows,
            preferred_element_type=jnp.float32,
        )
        new_acc = run_acc * jnp.transpose(correction)[..., None] + added
        return (new_max, new_total, new_acc)

    def step_latent(carry, blocks):
        key_nope, value_rows = expand(blocks[0])
        return attend_block(carry, key_nope, value_rows, blocks[1])

    initial = (
        jnp.full((local_heads, tok_rows), neg_large, jnp.float32),
        jnp.zeros((local_heads, tok_rows), jnp.float32),
        jnp.zeros((tok_rows, local_heads, VDIM), jnp.float32),
    )
    gathered = lax.all_gather(
        jnp.concatenate([key_latent, key_rot], axis=1), "ep", axis=0, tiled=True
    )
    rank = key_latent.shape[1]
    final = fold_blocks(initial, (gathered[:, :rank], gathered[:, rank:]), step_latent)
    run_max, run_total, run_acc = final
    heads_out = (run_acc / jnp.transpose(run_total)[..., None]).astype(jnp.bfloat16)
    heads_out = heads_out.reshape(tok_rows, local_heads * VDIM)
    return lax.psum_scatter(
        jnp.dot(heads_out, w_out, preferred_element_type=jnp.float32).astype(jnp.bfloat16),
        "tp",
        scatter_dimension=0,
        tiled=True,
    )


def expert_half(tokens_b, ffn_gain, route_expert, route_weight, w_gate, w_up, w_down):
    tok_rows = tokens_b.shape[0]
    expert_count = lax.axis_size("ep")
    capacity = TOPK * tok_rows // expert_count
    normed = rms_scale(tokens_b, ffn_gain)
    copies = route_expert.reshape(tok_rows * TOPK)
    chosen = (copies[:, None] == jnp.arange(expert_count, dtype=jnp.int32)[None, :]).astype(
        jnp.int32
    )
    earlier = jnp.cumsum(chosen, axis=0) - chosen
    slot_index = jnp.sum(earlier * chosen, axis=1)
    target = copies * capacity + slot_index
    source_row = (
        jnp.zeros((expert_count * capacity,), jnp.int32)
        .at[target]
        .set(jnp.arange(tok_rows * TOPK, dtype=jnp.int32) // TOPK)
    )
    outgoing = jnp.take(normed, source_row, axis=0)
    share_cols = outgoing.shape[1] // lax.axis_size("tp")
    own_cols = lax.dynamic_slice_in_dim(outgoing, lax.axis_index("tp") * share_cols, share_cols, 1)
    arrived = lax.all_to_all(own_cols, "ep", split_axis=0, concat_axis=0, tiled=True)
    member = lax.all_gather(arrived, "tp", axis=1, tiled=True)
    gate_rows = w_gate[0]
    up_rows = w_up[0]
    gate_act = jnp.dot(member, gate_rows, preferred_element_type=jnp.float32)
    up_act = jnp.dot(member, up_rows, preferred_element_type=jnp.float32)
    hidden = (jax.nn.silu(gate_act) * up_act).astype(jnp.bfloat16)
    partial_term = jnp.dot(hidden, w_down[0], preferred_element_type=jnp.float32)
    shared = lax.psum_scatter(
        partial_term.astype(jnp.bfloat16), "tp", scatter_dimension=1, tiled=True
    )
    returned = lax.all_to_all(shared, "ep", split_axis=0, concat_axis=0, tiled=True)
    picked = (
        jnp.take(returned, target, axis=0)
        .astype(jnp.float32)
        .reshape(tok_rows, TOPK, returned.shape[1])
    )
    combined = jnp.sum(picked * route_weight[:, :, None], axis=1)
    return combined.astype(jnp.bfloat16)


def flip(index, distance):
    low = index % 2
    high = index // 2
    if distance % 2 == 1:
        low = 1 - low
    if distance // 2 == 1:
        high = 1 - high
    return high * 2 + low


def expert_kernel(
    tokens_hbm,
    gain_hbm,
    route_hbm,
    weight_hbm,
    gate_hbm,
    up_hbm,
    down_hbm,
    query_hbm,
    latent_hbm,
    rope_hbm,
    query_gain_hbm,
    key_gain_hbm,
    w_query_hbm,
    w_rope_hbm,
    w_key_hbm,
    w_value_hbm,
    w_out_hbm,
    moe_ref,
    mixer_ref,
    tokens_ref,
    gain_ref,
    route_ref,
    share_ref,
    query_ref,
    latent_ref,
    rope_ref,
    query_gain_ref,
    key_gain_ref,
    w_query_ref,
    w_rope_ref,
    w_key_ref,
    w_value_ref,
    w_out_ref,
    order_ref,
    back_ref,
    weight_ref,
    weight_in,
    column_ref,
    scale_ref,
    outgoing_ref,
    member_ref,
    gate_ref,
    up_ref,
    down_ref,
    pair_send,
    pair_keep,
    pair_recv,
    first_send,
    first_keep,
    first_recv,
    second_send,
    second_keep,
    second_recv,
    fin_send,
    fin_ref,
    keys_ref,
    turns_ref,
    query_nope_ref,
    query_turn_ref,
    heads_ref,
    mixed_ref,
    mixed_in,
    joint_send,
    joint_recv,
    token_sem,
    load_sem,
    z_send,
    z_recv,
    x_send,
    x_recv,
    y_send,
    y_recv,
    c_send,
    c_recv,
    p_send,
    p_recv,
    f_send,
    f_recv,
    s_send,
    s_recv,
    o_send,
    o_recv,
    w_send,
    w_recv,
    kz_send,
    kz_recv,
    kx_send,
    kx_recv,
    kc_send,
    kc_recv,
    a_send,
    a_recv,
    j_send,
    j_recv,
):
    ep = lax.axis_index("ep")
    tp = lax.axis_index("tp")
    z, x = ep // 2, ep % 2
    y, c = tp // 2, tp % 2
    rows, half = outgoing_ref.shape[1:]
    lines_of = rows // HALVES
    tok_rows = tokens_ref.shape[0]
    share = fin_ref.shape[2]

    def sides(eighths):
        spare = half * eighths // 8
        kept = pl.ds(pl.multiple_of(y * spare, 128), half - spare)
        return kept, pl.ds(pl.multiple_of(y * (half - spare), 128), spare)

    def carried(u):
        return sides(Z_SPARES[u])[0]

    def forwarded(u):
        return sides(X_SPARES[u])[0]

    def passed(u, rel):
        return sides((Z_SPARES if rel == 0 else X_SPARES)[u])[1]

    at_end = (z == 0) | (z == GROUPS - 1)

    def at_z(distance):
        return {"ep": flip(z, distance) * 2 + x, "tp": tp}

    at_x = {"ep": z * 2 + 1 - x, "tp": tp}
    at_y = {"ep": ep, "tp": (1 - y) * 2 + c}
    at_c = {"ep": ep, "tp": y * 2 + 1 - c}

    barrier = pltpu.get_barrier_semaphore()
    for peer in (at_z(1), at_z(2), at_z(3), at_x, at_y, at_c):
        pl.semaphore_signal(barrier, inc=1, device_id=peer, device_id_type=MESH)

    loads = {}

    def load(name, source, target):
        loads[name] = pltpu.make_async_copy(source, target, load_sem.at[len(loads)])
        loads[name].start()

    load("route", route_hbm, route_ref)
    token_loads = []
    for k in range(4):
        lines = pl.ds(k * (tok_rows // 4), tok_rows // 4)
        token_loads.append(
            pltpu.make_async_copy(tokens_hbm.at[lines], tokens_ref.at[lines], token_sem.at[k])
        )
        token_loads[k].start()
    load("gain", gain_hbm, gain_ref)

    def load_rest():
        load("share", weight_hbm, share_ref)
        load("gate", gate_hbm.at[0], gate_ref)
        load("up", up_hbm.at[0], up_ref)
        for t in range(4):
            load(("down", t), down_hbm.at[0, :, pl.ds(t * share, share)], down_ref.at[t])
        load("key_gain", key_gain_hbm, key_gain_ref)
        load("latent", latent_hbm, latent_ref)
        load("rope", rope_hbm, rope_ref)
        load("query_gain", query_gain_hbm, query_gain_ref)
        load("query", query_hbm, query_ref)
        load("w_query", w_query_hbm, w_query_ref)
        load("w_rope", w_rope_hbm, w_rope_ref)
        load("w_key", w_key_hbm, w_key_ref)
        load("w_value", w_value_hbm, w_value_ref)
        load("w_out", w_out_hbm, w_out_ref)

    def dot(left, right):
        return jnp.dot(left, right, preferred_element_type=jnp.float32)

    def dot_lanes(left, right):
        return lax.dot_general(
            left, right, (((1,), (1,)), ((), ())), preferred_element_type=jnp.float32
        )

    def wide(value):
        return value.astype(jnp.float32)

    def scaled(values_in, gain):
        widened = wide(values_in)
        mean = jnp.mean(widened * widened, axis=-1, keepdims=True)
        return (widened * lax.rsqrt(mean + epsilon) * gain).astype(jnp.bfloat16)

    def iota(shape, dim):
        return lax.broadcasted_iota(jnp.int32, shape, dim)

    def group_lines(group):
        return pl.ds(pl.multiple_of(group * rows, rows), rows)

    before = jnp.where(iota((tok_rows, tok_rows), 0) < iota((tok_rows, tok_rows), 1), 1.0, 0.0)
    before = before.astype(jnp.bfloat16)
    loads["route"].wait()
    first = route_ref[0:1, :]
    group = jnp.zeros_like(first)
    for g in range(1, GROUPS):
        group = group + (first >= g * TOPK).astype(jnp.int32)
    picks = jnp.broadcast_to(group, (8, tok_rows)) == iota((8, tok_rows), 0)
    picks = jnp.where(picks, 1.0, 0.0)
    earlier = dot(picks.astype(jnp.bfloat16), before)
    rank_of = jnp.sum(earlier * picks, axis=0, keepdims=True).astype(jnp.int32)
    place = group * rows + rank_of
    for g in range(GROUPS):
        hit = jnp.broadcast_to(place, (rows, tok_rows)) == iota((rows, tok_rows), 0) + g * rows
        order_ref[g * rows : (g + 1) * rows, :] = jnp.where(hit, 1.0, 0.0).astype(jnp.bfloat16)

    def split(value):
        top = value.astype(jnp.bfloat16)
        rest = value - wide(top)
        middle = rest.astype(jnp.bfloat16)
        return wide(top), wide(middle), rest - wide(middle)

    width = tokens_ref.shape[1]
    for k in range(4):
        token_loads[k].wait()
        lines = slice(k * (tok_rows // 4), (k + 1) * (tok_rows // 4))
        squares = jnp.zeros((tok_rows // 4, 128), jnp.float32)
        for j in range(width // 128):
            widened = wide(tokens_ref[lines, j * 128 : (j + 1) * 128])
            squares = squares + widened * widened
        mean = jnp.sum(squares, axis=-1, keepdims=True) * (1.0 / width)
        lane = iota(squares.shape, 1)
        table = jnp.zeros(squares.shape, jnp.float32)
        for j, value in enumerate(split(lax.rsqrt(mean + epsilon))):
            table = jnp.where(lane == j, jnp.broadcast_to(value, table.shape), table)
        scale_ref[lines, :] = table.astype(jnp.bfloat16)
    loads["gain"].wait()
    load_rest()

    def remote(source, target, send, recv, peer):
        return pltpu.make_async_remote_copy(
            src_ref=source,
            dst_ref=target,
            send_sem=send,
            recv_sem=recv,
            device_id=peer,
            device_id_type=MESH,
        )

    def lines_at(u):
        return pl.ds(u % HALVES * lines_of, lines_of)

    def block_at(u):
        return flip(z, u // HALVES)

    def line_at(rel):
        return x if rel == 0 else 1 - x

    def z_copy(u):
        return remote(
            outgoing_ref.at[block_at(u), lines_at(u), carried(u)],
            member_ref.at[c, z, x, lines_at(u), carried(u)],
            z_send.at[u],
            z_recv.at[u],
            at_z(u // HALVES),
        )

    def w_copy(d):
        return remote(
            weight_ref.at[flip(z, d)], weight_in.at[z], w_send.at[d], w_recv.at[d], at_z(d)
        )

    def x_copy(u):
        piece = member_ref.at[c, block_at(u), x, lines_at(u), forwarded(u)]
        return remote(piece, piece, x_send.at[u], x_recv.at[u], at_x)

    def y_copy(u, rel):
        piece = member_ref.at[c, block_at(u), line_at(rel), lines_at(u), passed(u, rel)]
        k = 2 * u + rel
        return remote(piece, piece, y_send.at[k], y_recv.at[k], at_y)

    def c_copy(u, rel):
        piece = member_ref.at[c, block_at(u), line_at(rel), lines_at(u)]
        k = 2 * u + rel
        return remote(piece, piece, c_send.at[k], c_recv.at[k], at_c)

    def p_copy(u):
        return remote(pair_send.at[u], pair_recv.at[u], p_send.at[u], p_recv.at[u], at_c)

    def x_leads(u):
        return u in X_LEADS

    def f_copy(u):
        peer = at_x if x_leads(u) else at_y
        return remote(first_send.at[u], first_recv.at[u], f_send.at[u], f_recv.at[u], peer)

    def s_copy(u):
        peer = at_y if x_leads(u) else at_x
        return remote(second_send.at[u], second_recv.at[u], s_send.at[u], s_recv.at[u], peer)

    def o_copy(u):
        return remote(
            fin_send.at[u],
            fin_ref.at[z, lines_at(u)],
            o_send.at[u],
            o_recv.at[u],
            at_z(u // HALVES),
        )

    def key_pair(view, send, recv, k, peer):
        return [
            remote(ref, ref, send.at[2 * k + i], recv.at[2 * k + i], peer)
            for i, ref in enumerate(view)
        ]

    def kz_copy(d):
        view = (keys_ref.at[z, x, c], turns_ref.at[z, x, c])
        return key_pair(view, kz_send, kz_recv, d, at_z(d))

    def kx_copy(d):
        view = (keys_ref.at[flip(z, d), x, c], turns_ref.at[flip(z, d), x, c])
        return key_pair(view, kx_send, kx_recv, d, at_x)

    def kc_copy(d):
        if d == 0:
            view = (keys_ref.at[z, 1 - x, c], turns_ref.at[z, 1 - x, c])
        else:
            view = (keys_ref.at[flip(z, d), :, c], turns_ref.at[flip(z, d), :, c])
        return key_pair(view, kc_send, kc_recv, d, at_c)

    def a_copy(yy):
        return remote(
            mixed_ref.at[yy * 2 + 1 - c], mixed_in.at[yy], a_send.at[yy], a_recv.at[yy], at_c
        )

    def j_copy():
        return remote(joint_send, joint_recv, j_send.at[0], j_recv.at[0], at_y)

    started = []

    def copies_of(maker, args):
        made = maker(*args)
        return made if isinstance(made, list) else [made]

    def start(maker, *args):
        for copy in copies_of(maker, args):
            copy.start()
        if (maker, args) not in started:
            started.append((maker, args))

    def arrive(maker, *args):
        for copy in copies_of(maker, args):
            copy.wait_recv()

    def scale_of(group_index):
        table = dot(order_ref[group_lines(group_index), :], scale_ref[...])
        return jnp.sum(table, axis=-1, keepdims=True)

    def permuted(group_index, scale, first_col, cols):
        place_of = pl.ds(pl.multiple_of(first_col, 128), cols)
        picked = dot(order_ref[group_lines(group_index), :], tokens_ref[:, place_of])
        return (picked * scale * gain_ref[:, place_of]).astype(jnp.bfloat16)

    def make_units(d):
        eighths = min(Z_SPARES[d * HALVES + h] for h in range(HALVES))
        spare = half * eighths // 8
        outgoing_ref[flip(z, d), :, sides(eighths)[0]] = permuted(
            flip(z, d), scale_of(flip(z, d)), c * half + y * spare, half - spare
        )

    def make_own():
        scale = scale_of(z)
        for part in range(2):
            member_ref[part, z, x] = permuted(z, scale, part * half, half)

    made = set()
    for u in SENDS:
        d = u // HALVES
        if d not in made:
            if d > 0:
                make_units(d)
            else:
                make_own()
            if not made:
                pl.semaphore_wait(barrier, 6)
            made.add(d)
        if d > 0:
            start(z_copy, u)
        else:
            start(x_copy, u)

    def send_weights():
        loads["share"].wait()
        first_is_even = picks_even(route_ref[0:1, :])
        even = jnp.where(first_is_even, share_ref[0:1, :], share_ref[1:2, :])
        odd = jnp.where(first_is_even, share_ref[1:2, :], share_ref[0:1, :])
        line = iota((8, tok_rows), 0)
        table = jnp.zeros((8, tok_rows), jnp.float32)
        for k, value in enumerate(split(even) + split(odd)):
            table = jnp.where(line == k, jnp.broadcast_to(value, table.shape), table)
        table = table.astype(jnp.bfloat16)
        for g in range(GROUPS):
            weight_ref[g] = dot_lanes(table, order_ref[g * rows : (g + 1) * rows, :])
        for d in (1, 3, 2):
            start(w_copy, d)

    def picks_even(chosen):
        odd = jnp.zeros(chosen.shape, jnp.bool_)
        for e in range(1, GROUPS * TOPK, TOPK):
            odd = odd | (chosen == e)
        return jnp.logical_not(odd)

    def set_columns(d):
        if d > 0:
            arrive(w_copy, d)
        tile = weight_ref[z] if d == 0 else weight_in[flip(z, d)]
        even = tile[0:1] + tile[1:2] + tile[2:3]
        odd = tile[3:4] + tile[4:5] + tile[5:6]
        for k, line in enumerate(
            (jnp.where(x == 0, even, odd), jnp.where(x == 0, odd, even))
        ):
            column_ref[d, k] = jnp.transpose(jnp.broadcast_to(line, (rows, rows)))

    attend_rows, rank = latent_ref.shape
    key_half = attend_rows // 2
    lanes = 2 * ROPE

    def tables():
        lane = iota((1, lanes), 1)
        pair = (lane & (ROPE - 1)) >> 1
        quarter = ROPE // 4
        inverse = jnp.zeros((1, lanes), jnp.float32)
        for j in range(quarter):
            rate = rotary_base ** (-2.0 * j / (ROPE // 2))
            inverse = jnp.where((pair & (quarter - 1)) == j, rate, inverse)
        position = (ep * attend_rows + iota((attend_rows, lanes), 0)).astype(jnp.float32)
        grid_row = jnp.floor(position * (1.0 / GRID_W))
        grid_col = position - grid_row * GRID_W
        angle = jnp.where(jnp.broadcast_to(pair, position.shape) < quarter, grid_row, grid_col)
        angle = angle * inverse
        return jnp.cos(angle), jnp.sin(angle)

    def swap_matrix():
        from_lane = iota((lanes, lanes), 0)
        to_lane = iota((lanes, lanes), 1)
        to_even = (to_lane & 1) == 0
        swap = jnp.where(to_even & (from_lane == to_lane + 1), -1.0, 0.0)
        swap = jnp.where(jnp.logical_not(to_even) & (from_lane == to_lane - 1), 1.0, swap)
        return swap.astype(jnp.bfloat16)

    def make_keys():
        cosine, sine = tables()
        swap = swap_matrix()
        low_lane = iota((key_half, lanes), 1) < ROPE
        for name in ("key_gain", "latent", "rope"):
            loads[name].wait()
        keys_ref[z, x] = scaled(latent_ref[...], key_gain_ref[...]).reshape(2, key_half, rank)
        twice = jnp.transpose(jnp.concatenate([wide(rope_ref[...])] * 2, axis=0))
        turned = twice * cosine + dot(twice.astype(jnp.bfloat16), swap) * sine
        packed = jnp.where(low_lane, turned[:key_half], turned[key_half:])
        turns_ref[z, x] = packed.astype(jnp.bfloat16).reshape(2, key_half // 2, lanes)
        start(kx_copy, 0)
        for d in (1, 3, 2):
            start(kz_copy, d)
        for name in ("query_gain", "query", "w_query", "w_rope"):
            loads[name].wait()
        query_normed = scaled(query_ref[...], query_gain_ref[...])
        query_nope_ref[...] = dot(query_normed, w_query_ref[...]).astype(jnp.bfloat16)
        swapped = dot(w_rope_ref[...], swap).astype(jnp.bfloat16)
        query_turn = dot(query_normed, w_rope_ref[...]) * cosine
        query_turn = query_turn + dot(query_normed, swapped) * sine
        low = iota((attend_rows, lanes), 1) < ROPE
        for head in range(2):
            own = jnp.where(low if head == 0 else jnp.logical_not(low), query_turn, 0.0)
            other = pltpu.roll(own, ROPE, 1)
            query_turn_ref[head, head] = own.astype(jnp.bfloat16)
            query_turn_ref[head, 1 - head] = other.astype(jnp.bfloat16)

    def make_back():
        for k in range(tok_rows // rows):
            spread = jnp.broadcast_to(wide(place[:, k * rows : (k + 1) * rows]), (rows, rows))
            spread = jnp.transpose(spread)
            for g in range(GROUPS):
                target = (iota((rows, rows), 1) + g * rows).astype(jnp.float32)
                hit = jnp.where(spread == target, 1.0, 0.0).astype(jnp.bfloat16)
                back_ref[g, k * rows : (k + 1) * rows, :] = hit

    def compute(u):
        low = member_ref[0, block_at(u), :, lines_at(u), :].reshape(2 * lines_of, half)
        high = member_ref[1, block_at(u), :, lines_at(u), :].reshape(2 * lines_of, half)

        def project(weights):
            return dot(low, weights[:half, :]) + dot(high, weights[half:, :])

        gate_act = project(gate_ref)
        up_act = project(up_ref)
        hidden = (gate_act / (1.0 + jnp.exp(-gate_act)) * up_act).astype(jnp.bfloat16)
        for yy in range(2):
            term = dot(hidden, down_ref[yy * 2 + 1 - c])
            pair_send[u, yy] = term.astype(jnp.bfloat16).reshape(2, lines_of, share)
        start(p_copy, u)
        for yy in range(2):
            term = dot(hidden, down_ref[yy * 2 + c])
            pair_keep[u, yy] = term.astype(jnp.bfloat16).reshape(2, lines_of, share)

    def weights_of(u):
        def columns(k):
            square = column_ref[u // HALVES, k, lines_at(u), :]
            return jnp.concatenate([square] * (share // rows), axis=1)

        return columns(0), columns(1)

    def attend():
        for name in ("w_key", "w_value", "w_out"):
            loads[name].wait()
        blocks = keys_ref.shape[0] * keys_ref.shape[1]
        latents = keys_ref[...].reshape(blocks * attend_rows, rank)
        turns = turns_ref[...].reshape(blocks * key_half, lanes)
        key_nope = dot(latents, w_key_ref[...]).astype(jnp.bfloat16)
        value_rows = dot(latents, w_value_ref[...]).astype(jnp.bfloat16)
        key_nope = key_nope.reshape(blocks, 2, key_half, key_nope.shape[1])
        value_rows = value_rows.reshape(blocks, 2, key_half, value_rows.shape[1])
        for head in range(w_query_ref.shape[1] // NOPE):
            own = slice(head * NOPE, (head + 1) * NOPE)
            scores = []
            for part in range(2):
                left = jnp.concatenate(
                    [query_nope_ref[:, own], query_turn_ref[head, part]], axis=1
                )
                keys = key_nope[:, part, :, own].reshape(blocks * key_half, NOPE)
                right = jnp.concatenate([keys, turns], axis=1)
                scores.append(dot_lanes(left, right) * (NOPE + ROPE) ** (-0.5))
            top = jnp.maximum(
                jnp.max(scores[0], axis=-1, keepdims=True),
                jnp.max(scores[1], axis=-1, keepdims=True),
            )
            totals = jnp.zeros(top.shape, jnp.float32)
            mixed = jnp.zeros((attend_rows, VDIM), jnp.float32)
            for part in range(2):
                raised = jnp.exp(scores[part] - top)
                totals = totals + jnp.sum(raised, axis=-1, keepdims=True)
                values = value_rows[:, part, :, own].reshape(blocks * key_half, VDIM)
                mixed = mixed + dot(raised.astype(jnp.bfloat16), values)
            heads_ref[:, own] = (mixed / totals).astype(jnp.bfloat16)
        for t in range(4):
            lines = slice(t * (attend_rows // 4), (t + 1) * (attend_rows // 4))
            mixed_ref[t] = dot(heads_ref[lines, :], w_out_ref[...]).astype(jnp.bfloat16)
        for yy in range(2):
            start(a_copy, yy)

    def attend_join():
        for yy in range(2):
            arrive(a_copy, yy)
        sums = wide(mixed_ref[(1 - y) * 2 + c]) + wide(mixed_in[1 - y])
        joint_send[...] = sums.astype(jnp.bfloat16)
        start(j_copy)

    def attend_last():
        arrive(j_copy)
        sums = wide(mixed_ref[y * 2 + c]) + wide(mixed_in[y]) + wide(joint_recv[...])
        mixer_ref[...] = sums.astype(jnp.bfloat16)

    def stage_first(u):
        arrive(p_copy, u)
        if x_leads(u):
            for yy in range(2):
                sums = wide(pair_keep[u, yy, 1 - x]) + wide(pair_recv[u, yy, 1 - x])
                first_send[u, yy] = sums.astype(jnp.bfloat16)
            start(f_copy, u)
            for yy in range(2):
                first_keep[u, yy] = wide(pair_keep[u, yy, x]) + wide(pair_recv[u, yy, x])
        else:
            for line in range(2):
                sums = wide(pair_keep[u, 1 - y, line]) + wide(pair_recv[u, 1 - y, line])
                first_send[u, line] = sums.astype(jnp.bfloat16)
            start(f_copy, u)
            for line in range(2):
                first_keep[u, line] = wide(pair_keep[u, y, line]) + wide(pair_recv[u, y, line])

    def stage_second(u):
        arrive(f_copy, u)
        if x_leads(u):
            mine, other = weights_of(u)
            sums = mine * first_keep[u, 1 - y] + other * wide(first_recv[u, 1 - y])
            second_send[u] = sums.astype(jnp.bfloat16)
            start(s_copy, u)
            second_keep[u] = mine * first_keep[u, y] + other * wide(first_recv[u, y])
        else:
            sums = first_keep[u, 1 - x] + wide(first_recv[u, 1 - x])
            second_send[u] = sums.astype(jnp.bfloat16)
            start(s_copy, u)
            sums = first_keep[u, x] + wide(first_recv[u, x])
            second_keep[u] = wide(sums.astype(jnp.bfloat16))

    def stage_last(u):
        arrive(s_copy, u)
        if x_leads(u):
            result = second_keep[u] + wide(second_recv[u])
        else:
            mine, other = weights_of(u)
            result = mine * second_keep[u] + other * wide(second_recv[u])
        if u // HALVES == 0:
            fin_ref[z, lines_at(u)] = result.astype(jnp.bfloat16)
        else:
            fin_send[u] = result.astype(jnp.bfloat16)
            start(o_copy, u)

    def from_z(u):
        arrive(z_copy, u)
        start(x_copy, u)
        if Z_SPARES[u] > 0:
            start(y_copy, u, 0)

    def from_x(u):
        arrive(x_copy, u)
        start(y_copy, u, 1)

    def from_y(u, rel):
        if rel == 1 or Z_SPARES[u] > 0:
            arrive(y_copy, u, rel)
        start(c_copy, u, rel)

    def gathered(u):
        for rel in range(2):
            if u // HALVES > 0 or rel > 0:
                arrive(c_copy, u, rel)

    def wait_weights():
        for name in ("gate", "up"):
            loads[name].wait()
        for t in range(4):
            loads[("down", t)].wait()

    def from_kz(d):
        arrive(kz_copy, d)
        start(kx_copy, d)

    def from_kx(d):
        arrive(kx_copy, d)
        start(kc_copy, d)

    def from_kc(d):
        arrive(kc_copy, d)

    added = []

    def give_back(d):
        if d > 0:
            for h in range(HALVES):
                arrive(o_copy, d * HALVES + h)
        term = dot(back_ref[flip(z, d)], fin_ref[flip(z, d)])
        if added:
            term = term + wide(moe_ref[...])
        added.append(d)
        moe_ref[...] = term.astype(jnp.bfloat16)

    steps = {
        "z": from_z,
        "x": from_x,
        "y": from_y,
        "g": gathered,
        "m": compute,
        "1": stage_first,
        "2": stage_second,
        "3": stage_last,
        "weights": send_weights,
        "columns": set_columns,
        "keys": make_keys,
        "back": make_back,
        "loaded": wait_weights,
        "kz": from_kz,
        "kx": from_kx,
        "kc": from_kc,
        "attend": attend,
        "join": attend_join,
        "last": attend_last,
        "b": give_back,
    }

    for item in SCHEDULE:
            where, text = "", item
            if item[0] in "<>":
                where, text = item[0], item[1:]
            name, *numbers = text.split(".")
            step = steps[name]
            values = [int(number) for number in numbers]
            if where == "":
                step(*values)
            else:
                pl.when(at_end if where == ">" else jnp.logical_not(at_end))(
                    functools.partial(step, *values)
                )
    for maker, args in started:
        for copy in copies_of(maker, args):
            copy.wait_send()


SCHEDULE = (
    ">z.2", ">x.0", "loaded", "<z.6", "<x.0", "<z.7", "<z.2", "<x.6", "<z.3", "<x.2", "<y.2.0",
    "<y.7.0", "<y.6.1", "x.1", ">z.6", ">z.3", ">y.1.1", "y.0.1", ">z.4", ">x.6", ">z.7", "y.6.0",
    "<x.3", "keys", ">z.5", ">y.6.1", "x.7", "<z.4", "g.6", "m.6", ">x.3", ">y.7.0", ">x.4",
    ">y.3.0", ">kz.1", "<z.5", "<y.3.1", "g.0", "m.0", ">kx.0", ">x.5", "<y.1.1", "<kz.1", "1.6",
    "<kz.3", "<y.3.0", "<y.7.1", "<kx.0", "<y.2.1", "weights", ">y.7.1", ">x.2", ">kz.2", ">y.5.0",
    ">kz.3", ">y.3.1", ">kx.1", "<x.4", "<x.5", "g.7", "m.7", "1.0", "<y.5.0", "<kz.2", "<y.4.0",
    "<kc.0", "<kx.1", "<y.4.1", "g.1", "m.1", ">kc.0", ">y.5.1", ">y.4.1", "1.7", "<y.5.1",
    "columns.3", ">y.4.0", "g.3", "m.3", "2.6", ">y.2.1", "columns.2", "g.5", "m.5", ">kx.2",
    ">y.2.0", "1.3", "g.4", "m.4", "1.5", "g.2", "m.2", "back", "3.6", "2.7", "<kc.1", "<kx.2",
    "1.4", "columns.1", "2.3", ">kx.3", "2.5", "1.2", "kc.2", "1.1", ">kc.3", ">kc.1", "<kx.3",
    "3.7", "<kc.3", "attend", "3.5", "2.4", "2.0", "columns.0", "3.3", "join", "2.2", "3.4", "3.0",
    "2.1", "b.3", "3.2", "3.1", "last", "b.0", "b.2", "b.1",
)


def expert_exchange(tokens_b, ffn_gain, route, share_of, w_gate, w_up, w_down, mixer_args):
    tok_rows, width = tokens_b.shape
    rows = tok_rows // GROUPS
    half = width // 2
    share = width // 4
    units = w_gate.shape[2]
    attend_rows, rank = mixer_args[1].shape
    head_cols = mixer_args[7].shape[1]
    rank_q = mixer_args[0].shape[1]
    count = GROUPS * HALVES
    part = rows // HALVES
    narrow, full = jnp.bfloat16, jnp.float32
    vmem = pl.BlockSpec(memory_space=pltpu.VMEM)
    anywhere = pl.BlockSpec(memory_space=pl.ANY)
    dma = pltpu.SemaphoreType.DMA
    operands = (
        tokens_b,
        ffn_gain.reshape(1, width),
        route,
        share_of,
        w_gate,
        w_up,
        w_down,
        *mixer_args,
    )
    return pl.pallas_call(
        expert_kernel,
        out_shape=(
            pltpu.VMEM((tok_rows, share), narrow),
            pltpu.VMEM((attend_rows // 4, width), narrow),
        ),
        in_specs=[anywhere] * len(operands),
        out_specs=(vmem, vmem),
        scratch_shapes=[
            pltpu.VMEM((tok_rows, width), narrow),
            pltpu.VMEM((1, width), full),
            pltpu.VMEM(route.shape, jnp.int32),
            pltpu.VMEM(share_of.shape, full),
            pltpu.VMEM((attend_rows, rank_q), narrow),
            pltpu.VMEM((attend_rows, rank), narrow),
            pltpu.VMEM((ROPE, attend_rows), narrow),
            pltpu.VMEM((1, rank_q), full),
            pltpu.VMEM((1, rank), full),
            pltpu.VMEM(mixer_args[5].shape, narrow),
            pltpu.VMEM(mixer_args[6].shape, narrow),
            pltpu.VMEM(mixer_args[7].shape, narrow),
            pltpu.VMEM(mixer_args[8].shape, narrow),
            pltpu.VMEM(mixer_args[9].shape, narrow),
            pltpu.VMEM((tok_rows, tok_rows), narrow),
            pltpu.VMEM((GROUPS, tok_rows, rows), narrow),
            pltpu.VMEM((GROUPS, 8, rows), full),
            pltpu.VMEM((GROUPS, 8, rows), full),
            pltpu.VMEM((GROUPS, 2, rows, rows), full),
            pltpu.VMEM((tok_rows, 128), narrow),
            pltpu.VMEM((GROUPS, rows, half), narrow),
            pltpu.VMEM((2, GROUPS, 2, rows, half), narrow),
            pltpu.VMEM((width, units), narrow),
            pltpu.VMEM((width, units), narrow),
            pltpu.VMEM((4, units, share), narrow),
            pltpu.VMEM((count, 2, 2, part, share), narrow),
            pltpu.VMEM((count, 2, 2, part, share), narrow),
            pltpu.VMEM((count, 2, 2, part, share), narrow),
            pltpu.VMEM((count, 2, part, share), narrow),
            pltpu.VMEM((count, 2, part, share), full),
            pltpu.VMEM((count, 2, part, share), narrow),
            pltpu.VMEM((count, part, share), narrow),
            pltpu.VMEM((count, part, share), full),
            pltpu.VMEM((count, part, share), narrow),
            pltpu.VMEM((count, part, share), narrow),
            pltpu.VMEM((GROUPS, rows, share), narrow),
            pltpu.VMEM((GROUPS, 2, 2, attend_rows // 2, rank), narrow),
            pltpu.VMEM((GROUPS, 2, 2, attend_rows // 4, 2 * ROPE), narrow),
            pltpu.VMEM((attend_rows, head_cols), narrow),
            pltpu.VMEM((2, 2, attend_rows, 2 * ROPE), narrow),
            pltpu.VMEM((attend_rows, head_cols), narrow),
            pltpu.VMEM((4, attend_rows // 4, width), narrow),
            pltpu.VMEM((2, attend_rows // 4, width), narrow),
            pltpu.VMEM((attend_rows // 4, width), narrow),
            pltpu.VMEM((attend_rows // 4, width), narrow),
            dma((4,)),
            dma((24,)),
        ]
        + [dma((count,))] * 4
        + [dma((2 * count,))] * 4
        + [dma((count,))] * 8
        + [dma((GROUPS,))] * 2
        + [dma((2 * GROUPS,))] * 6
        + [dma((2,))] * 4,
        compiler_params=pltpu.CompilerParams(
            collective_id=0, has_side_effects=True, vmem_limit_bytes=48 * 1024 * 1024
        ),
        cost_estimate=pl.CostEstimate(
            flops=40_000_000_000, bytes_accessed=8_000_000, transcendentals=0
        ),
        name="expert_exchange",
    )(*(pltpu.with_memory_space_constraint(operand, pltpu.HBM) for operand in operands))


def paired(mixer, tokens_b, ffn_gain, route_expert, route_weight, w_gate, w_up, w_down):
    query_latent, key_latent, rope_key, query_gain, key_gain = mixer[:5]
    mixer_args = (
        query_latent,
        key_latent,
        rope_key.T,
        query_gain.reshape(1, -1),
        key_gain.reshape(1, -1),
        *mixer[5:],
    )
    moe_out, mixer_out = expert_exchange(
        tokens_b, ffn_gain, route_expert.T, route_weight.T, w_gate, w_up, w_down, mixer_args
    )
    return (mixer_out, moe_out)


def body(
    query_latent,
    key_latent,
    rope_key,
    query_gain,
    key_gain,
    w_query,
    w_query_rope,
    w_key,
    w_value,
    w_out,
    tokens_b,
    ffn_gain,
    route_expert,
    route_weight,
    w_gate,
    w_up,
    w_down,
):
    mixer = (
        query_latent,
        key_latent,
        rope_key,
        query_gain,
        key_gain,
        w_query,
        w_query_rope,
        w_key,
        w_value,
        w_out,
    )
    experts = (tokens_b, ffn_gain, route_expert, route_weight, w_gate, w_up, w_down)
    if (
        lax.axis_size("ep") == GROUPS * TOPK
        and lax.axis_size("tp") == 4
        and GROUPS == 4
        and tokens_b.shape[0] == GROUPS * 128
        and w_query.shape[1] == 2 * NOPE
    ):
        return paired(mixer, *experts)
    return (mixer_half(*mixer), expert_half(*experts))


def solution(mesh):
    in_specs = (
        P("ep", None),
        P("ep", None),
        P("ep", None),
        P(),
        P(),
        P(None, "tp"),
        P(None, "tp"),
        P(None, "tp"),
        P(None, "tp"),
        P("tp", None),
        P("ep", None),
        P(),
        P("ep", None),
        P("ep", None),
        P("ep", None, "tp"),
        P("ep", None, "tp"),
        P("ep", "tp", None),
    )
    out_specs = (P(("ep", "tp"), None), P("ep", "tp"))
    return jax.shard_map(body, mesh=mesh, in_specs=in_specs, out_specs=out_specs, check_vma=False)
```

```python
import functools
import math

import jax
import jax.numpy as jnp
from jax import lax
from jax.experimental import pallas as pl
from jax.experimental.pallas import tpu as pltpu
from jax.sharding import PartitionSpec as P

NOPE = 128
ROPE = 64
VDIM = 128
GRID_W = 64
TOPK = 2
GROUPS = 4
MESH = pl.DeviceIdType.MESH
HALVES = 2
Z_SPARES = (0, 1, 4, 3, 4, 4, 4, 4)
X_SPARES = (3, 1, 4, 3, 4, 4, 4, 4)
X_LEADS = (1, 3, 4, 6)
SENDS = (2, 6, 3, 7, 0, 1, 4, 5)


epsilon = 1e-06
rotary_base = 10000.0
neg_large = -1e30


def rms_scale(values_in, gain):
    widened = values_in.astype(jnp.float32)
    normed = widened * lax.rsqrt(jnp.mean(widened * widened, axis=-1, keepdims=True) + epsilon)
    return (normed * gain).astype(jnp.bfloat16)


def rotary_tables(positions):
    half_width = ROPE // 2
    inverse = rotary_base ** (-jnp.arange(0, half_width, 2, dtype=jnp.float32) / half_width)
    grid_row = (positions // GRID_W).astype(jnp.float32)
    grid_col = (positions % GRID_W).astype(jnp.float32)
    angle = jnp.concatenate([grid_row[:, None] * inverse, grid_col[:, None] * inverse], axis=-1)
    return (jnp.cos(angle), jnp.sin(angle))


def rotate(values_in, cosine, sine):
    even_part = values_in[..., 0::2]
    odd_part = values_in[..., 1::2]
    turned = jnp.stack(
        [even_part * cosine - odd_part * sine, even_part * sine + odd_part * cosine], axis=-1
    )
    return turned.reshape(values_in.shape)


def fold_blocks(carry, members, step_fn):
    piece_rows = members[0].shape[0]
    block_rows = math.gcd(piece_rows, 1024)
    if block_rows == piece_rows:
        return step_fn(carry, members)
    stacked = tuple(
        (
            member.reshape((piece_rows // block_rows, block_rows) + member.shape[1:])
            for member in members
        )
    )

    def scan_step(inner_carry, blocks):
        return (step_fn(inner_carry, blocks), None)

    result, unused = lax.scan(scan_step, carry, stacked)
    return result


def mixer_half(
    query_latent,
    key_latent,
    rope_key,
    query_gain,
    key_gain,
    w_query,
    w_query_rope,
    w_key,
    w_value,
    w_out,
):
    tok_rows = query_latent.shape[0]
    local_heads = w_query.shape[1] // NOPE
    positions = lax.axis_index("ep") * tok_rows + jnp.arange(tok_rows, dtype=jnp.int32)
    cosine, sine = rotary_tables(positions)
    query_normed = rms_scale(query_latent, query_gain)
    query_nope = jnp.dot(query_normed, w_query, preferred_element_type=jnp.float32).astype(
        jnp.bfloat16
    )
    query_nope = query_nope.reshape(tok_rows, local_heads, NOPE)
    query_rot = jnp.dot(query_normed, w_query_rope, preferred_element_type=jnp.float32)
    query_rot = rotate(
        query_rot.reshape(tok_rows, local_heads, ROPE), cosine[:, None, :], sine[:, None, :]
    )
    query_rot = query_rot.astype(jnp.bfloat16)
    key_rot = rotate(rope_key.astype(jnp.float32), cosine, sine).astype(jnp.bfloat16)
    score_scale = (NOPE + ROPE) ** (-0.5)

    def expand(latent_rows):
        latent_count = latent_rows.shape[0]
        key_normed = rms_scale(latent_rows, key_gain)
        key_nope = jnp.dot(key_normed, w_key, preferred_element_type=jnp.float32).astype(
            jnp.bfloat16
        )
        value_rows = jnp.dot(key_normed, w_value, preferred_element_type=jnp.float32).astype(
            jnp.bfloat16
        )
        return (
            key_nope.reshape(latent_count, local_heads, NOPE),
            value_rows.reshape(latent_count, local_heads, VDIM),
        )

    def attend_block(carry, key_nope, value_rows, key_turn):
        run_max, run_total, run_acc = carry
        scores = jnp.einsum(
            "qhd,khd->hqk", query_nope, key_nope, preferred_element_type=jnp.float32
        )
        scores = scores + jnp.einsum(
            "qhd,kd->hqk", query_rot, key_turn, preferred_element_type=jnp.float32
        )
        scores = scores * score_scale
        new_max = jnp.maximum(run_max, jnp.max(scores, axis=-1))
        correction = jnp.exp(run_max - new_max)
        weights = jnp.exp(scores - new_max[..., None])
        new_total = run_total * correction + jnp.sum(weights, axis=-1)
        added = jnp.einsum(
            "hqk,khd->qhd",
            weights.astype(jnp.bfloat16),
            value_rows,
            preferred_element_type=jnp.float32,
        )
        new_acc = run_acc * jnp.transpose(correction)[..., None] + added
        return (new_max, new_total, new_acc)

    def step_latent(carry, blocks):
        key_nope, value_rows = expand(blocks[0])
        return attend_block(carry, key_nope, value_rows, blocks[1])

    initial = (
        jnp.full((local_heads, tok_rows), neg_large, jnp.float32),
        jnp.zeros((local_heads, tok_rows), jnp.float32),
        jnp.zeros((tok_rows, local_heads, VDIM), jnp.float32),
    )
    gathered = lax.all_gather(
        jnp.concatenate([key_latent, key_rot], axis=1), "ep", axis=0, tiled=True
    )
    rank = key_latent.shape[1]
    final = fold_blocks(initial, (gathered[:, :rank], gathered[:, rank:]), step_latent)
    run_max, run_total, run_acc = final
    heads_out = (run_acc / jnp.transpose(run_total)[..., None]).astype(jnp.bfloat16)
    heads_out = heads_out.reshape(tok_rows, local_heads * VDIM)
    return lax.psum_scatter(
        jnp.dot(heads_out, w_out, preferred_element_type=jnp.float32).astype(jnp.bfloat16),
        "tp",
        scatter_dimension=0,
        tiled=True,
    )


def expert_half(tokens_b, ffn_gain, route_expert, route_weight, w_gate, w_up, w_down):
    tok_rows = tokens_b.shape[0]
    expert_count = lax.axis_size("ep")
    capacity = TOPK * tok_rows // expert_count
    normed = rms_scale(tokens_b, ffn_gain)
    copies = route_expert.reshape(tok_rows * TOPK)
    chosen = (copies[:, None] == jnp.arange(expert_count, dtype=jnp.int32)[None, :]).astype(
        jnp.int32
    )
    earlier = jnp.cumsum(chosen, axis=0) - chosen
    slot_index = jnp.sum(earlier * chosen, axis=1)
    target = copies * capacity + slot_index
    source_row = (
        jnp.zeros((expert_count * capacity,), jnp.int32)
        .at[target]
        .set(jnp.arange(tok_rows * TOPK, dtype=jnp.int32) // TOPK)
    )
    outgoing = jnp.take(normed, source_row, axis=0)
    share_cols = outgoing.shape[1] // lax.axis_size("tp")
    own_cols = lax.dynamic_slice_in_dim(outgoing, lax.axis_index("tp") * share_cols, share_cols, 1)
    arrived = lax.all_to_all(own_cols, "ep", split_axis=0, concat_axis=0, tiled=True)
    member = lax.all_gather(arrived, "tp", axis=1, tiled=True)
    gate_rows = w_gate[0]
    up_rows = w_up[0]
    gate_act = jnp.dot(member, gate_rows, preferred_element_type=jnp.float32)
    up_act = jnp.dot(member, up_rows, preferred_element_type=jnp.float32)
    hidden = (jax.nn.silu(gate_act) * up_act).astype(jnp.bfloat16)
    partial_term = jnp.dot(hidden, w_down[0], preferred_element_type=jnp.float32)
    shared = lax.psum_scatter(
        partial_term.astype(jnp.bfloat16), "tp", scatter_dimension=1, tiled=True
    )
    returned = lax.all_to_all(shared, "ep", split_axis=0, concat_axis=0, tiled=True)
    picked = (
        jnp.take(returned, target, axis=0)
        .astype(jnp.float32)
        .reshape(tok_rows, TOPK, returned.shape[1])
    )
    combined = jnp.sum(picked * route_weight[:, :, None], axis=1)
    return combined.astype(jnp.bfloat16)


def flip(index, distance):
    low = index % 2
    high = index // 2
    if distance % 2 == 1:
        low = 1 - low
    if distance // 2 == 1:
        high = 1 - high
    return high * 2 + low


def expert_kernel(
    tokens_hbm,
    gain_hbm,
    route_hbm,
    weight_hbm,
    gate_hbm,
    up_hbm,
    down_hbm,
    query_hbm,
    latent_hbm,
    rope_hbm,
    query_gain_hbm,
    key_gain_hbm,
    w_query_hbm,
    w_rope_hbm,
    w_key_hbm,
    w_value_hbm,
    w_out_hbm,
    moe_ref,
    mixer_ref,
    tokens_ref,
    gain_ref,
    route_ref,
    share_ref,
    query_ref,
    latent_ref,
    rope_ref,
    query_gain_ref,
    key_gain_ref,
    w_query_ref,
    w_rope_ref,
    w_key_ref,
    w_value_ref,
    w_out_ref,
    order_ref,
    back_ref,
    weight_ref,
    weight_in,
    column_ref,
    scale_ref,
    outgoing_ref,
    member_ref,
    gate_ref,
    up_ref,
    down_ref,
    pair_send,
    pair_keep,
    pair_recv,
    first_send,
    first_keep,
    first_recv,
    second_send,
    second_keep,
    second_recv,
    fin_send,
    fin_ref,
    keys_ref,
    turns_ref,
    query_nope_ref,
    query_turn_ref,
    heads_ref,
    mixed_ref,
    mixed_in,
    joint_send,
    joint_recv,
    token_sem,
    load_sem,
    z_send,
    z_recv,
    x_send,
    x_recv,
    y_send,
    y_recv,
    c_send,
    c_recv,
    p_send,
    p_recv,
    f_send,
    f_recv,
    s_send,
    s_recv,
    o_send,
    o_recv,
    w_send,
    w_recv,
    kz_send,
    kz_recv,
    kx_send,
    kx_recv,
    kc_send,
    kc_recv,
    a_send,
    a_recv,
    j_send,
    j_recv,
):
    ep = lax.axis_index("ep")
    tp = lax.axis_index("tp")
    z, x = ep // 2, ep % 2
    y, c = tp // 2, tp % 2
    rows, half = outgoing_ref.shape[1:]
    lines_of = rows // HALVES
    tok_rows = tokens_ref.shape[0]
    share = fin_ref.shape[2]

    def sides(eighths):
        spare = half * eighths // 8
        kept = pl.ds(pl.multiple_of(y * spare, 128), half - spare)
        return kept, pl.ds(pl.multiple_of(y * (half - spare), 128), spare)

    def carried(u):
        return sides(Z_SPARES[u])[0]

    def forwarded(u):
        return sides(X_SPARES[u])[0]

    def passed(u, rel):
        return sides((Z_SPARES if rel == 0 else X_SPARES)[u])[1]

    at_end = (z == 0) | (z == GROUPS - 1)

    def at_z(distance):
        return {"ep": flip(z, distance) * 2 + x, "tp": tp}

    at_x = {"ep": z * 2 + 1 - x, "tp": tp}
    at_y = {"ep": ep, "tp": (1 - y) * 2 + c}
    at_c = {"ep": ep, "tp": y * 2 + 1 - c}

    barrier = pltpu.get_barrier_semaphore()
    for peer in (at_z(1), at_z(2), at_z(3), at_x, at_y, at_c):
        pl.semaphore_signal(barrier, inc=1, device_id=peer, device_id_type=MESH)

    loads = {}

    def load(name, source, target):
        loads[name] = pltpu.make_async_copy(source, target, load_sem.at[len(loads)])
        loads[name].start()

    load("route", route_hbm, route_ref)
    token_loads = []
    for k in range(4):
        lines = pl.ds(k * (tok_rows // 4), tok_rows // 4)
        token_loads.append(
            pltpu.make_async_copy(tokens_hbm.at[lines], tokens_ref.at[lines], token_sem.at[k])
        )
        token_loads[k].start()
    load("gain", gain_hbm, gain_ref)

    def load_rest():
        load("share", weight_hbm, share_ref)
        load("gate", gate_hbm.at[0], gate_ref)
        load("up", up_hbm.at[0], up_ref)
        for t in range(4):
            load(("down", t), down_hbm.at[0, :, pl.ds(t * share, share)], down_ref.at[t])
        load("key_gain", key_gain_hbm, key_gain_ref)
        load("latent", latent_hbm, latent_ref)
        load("rope", rope_hbm, rope_ref)
        load("query_gain", query_gain_hbm, query_gain_ref)
        load("query", query_hbm, query_ref)
        load("w_query", w_query_hbm, w_query_ref)
        load("w_rope", w_rope_hbm, w_rope_ref)
        load("w_key", w_key_hbm, w_key_ref)
        load("w_value", w_value_hbm, w_value_ref)
        load("w_out", w_out_hbm, w_out_ref)

    def dot(left, right):
        return jnp.dot(left, right, preferred_element_type=jnp.float32)

    def dot_lanes(left, right):
        return lax.dot_general(
            left, right, (((1,), (1,)), ((), ())), preferred_element_type=jnp.float32
        )

    def wide(value):
        return value.astype(jnp.float32)

    def scaled(values_in, gain):
        widened = wide(values_in)
        mean = jnp.mean(widened * widened, axis=-1, keepdims=True)
        return (widened * lax.rsqrt(mean + epsilon) * gain).astype(jnp.bfloat16)

    def iota(shape, dim):
        return lax.broadcasted_iota(jnp.int32, shape, dim)

    def group_lines(group):
        return pl.ds(pl.multiple_of(group * rows, rows), rows)

    before = jnp.where(iota((tok_rows, tok_rows), 0) < iota((tok_rows, tok_rows), 1), 1.0, 0.0)
    before = before.astype(jnp.bfloat16)
    loads["route"].wait()
    first = route_ref[0:1, :]
    group = jnp.zeros_like(first)
    for g in range(1, GROUPS):
        group = group + (first >= g * TOPK).astype(jnp.int32)
    picks = jnp.broadcast_to(group, (8, tok_rows)) == iota((8, tok_rows), 0)
    picks = jnp.where(picks, 1.0, 0.0)
    earlier = dot(picks.astype(jnp.bfloat16), before)
    rank_of = jnp.sum(earlier * picks, axis=0, keepdims=True).astype(jnp.int32)
    place = group * rows + rank_of
    for g in range(GROUPS):
        hit = jnp.broadcast_to(place, (rows, tok_rows)) == iota((rows, tok_rows), 0) + g * rows
        order_ref[g * rows : (g + 1) * rows, :] = jnp.where(hit, 1.0, 0.0).astype(jnp.bfloat16)

    def split(value):
        top = value.astype(jnp.bfloat16)
        rest = value - wide(top)
        middle = rest.astype(jnp.bfloat16)
        return wide(top), wide(middle), rest - wide(middle)

    width = tokens_ref.shape[1]
    for k in range(4):
        token_loads[k].wait()
        lines = slice(k * (tok_rows // 4), (k + 1) * (tok_rows // 4))
        squares = jnp.zeros((tok_rows // 4, 128), jnp.float32)
        for j in range(width // 128):
            widened = wide(tokens_ref[lines, j * 128 : (j + 1) * 128])
            squares = squares + widened * widened
        mean = jnp.sum(squares, axis=-1, keepdims=True) * (1.0 / width)
        lane = iota(squares.shape, 1)
        table = jnp.zeros(squares.shape, jnp.float32)
        for j, value in enumerate(split(lax.rsqrt(mean + epsilon))):
            table = jnp.where(lane == j, jnp.broadcast_to(value, table.shape), table)
        scale_ref[lines, :] = table.astype(jnp.bfloat16)
    loads["gain"].wait()
    load_rest()

    def remote(source, target, send, recv, peer):
        return pltpu.make_async_remote_copy(
            src_ref=source,
            dst_ref=target,
            send_sem=send,
            recv_sem=recv,
            device_id=peer,
            device_id_type=MESH,
        )

    def lines_at(u):
        return pl.ds(u % HALVES * lines_of, lines_of)

    def block_at(u):
        return flip(z, u // HALVES)

    def line_at(rel):
        return x if rel == 0 else 1 - x

    def z_copy(u):
        return remote(
            outgoing_ref.at[block_at(u), lines_at(u), carried(u)],
            member_ref.at[c, z, x, lines_at(u), carried(u)],
            z_send.at[u],
            z_recv.at[u],
            at_z(u // HALVES),
        )

    def w_copy(d):
        return remote(
            weight_ref.at[flip(z, d)], weight_in.at[z], w_send.at[d], w_recv.at[d], at_z(d)
        )

    def x_copy(u):
        piece = member_ref.at[c, block_at(u), x, lines_at(u), forwarded(u)]
        return remote(piece, piece, x_send.at[u], x_recv.at[u], at_x)

    def y_copy(u, rel):
        piece = member_ref.at[c, block_at(u), line_at(rel), lines_at(u), passed(u, rel)]
        k = 2 * u + rel
        return remote(piece, piece, y_send.at[k], y_recv.at[k], at_y)

    def c_copy(u, rel):
        piece = member_ref.at[c, block_at(u), line_at(rel), lines_at(u)]
        k = 2 * u + rel
        return remote(piece, piece, c_send.at[k], c_recv.at[k], at_c)

    def p_copy(u):
        return remote(pair_send.at[u], pair_recv.at[u], p_send.at[u], p_recv.at[u], at_c)

    def x_leads(u):
        return u in X_LEADS

    def f_copy(u):
        peer = at_x if x_leads(u) else at_y
        return remote(first_send.at[u], first_recv.at[u], f_send.at[u], f_recv.at[u], peer)

    def s_copy(u):
        peer = at_y if x_leads(u) else at_x
        return remote(second_send.at[u], second_recv.at[u], s_send.at[u], s_recv.at[u], peer)

    def o_copy(u):
        return remote(
            fin_send.at[u],
            fin_ref.at[z, lines_at(u)],
            o_send.at[u],
            o_recv.at[u],
            at_z(u // HALVES),
        )

    def key_pair(view, send, recv, k, peer):
        return [
            remote(ref, ref, send.at[2 * k + i], recv.at[2 * k + i], peer)
            for i, ref in enumerate(view)
        ]

    def kz_copy(d):
        view = (keys_ref.at[z, x, c], turns_ref.at[z, x, c])
        return key_pair(view, kz_send, kz_recv, d, at_z(d))

    def kx_copy(d):
        view = (keys_ref.at[flip(z, d), x, c], turns_ref.at[flip(z, d), x, c])
        return key_pair(view, kx_send, kx_recv, d, at_x)

    def kc_copy(d):
        if d == 0:
            view = (keys_ref.at[z, 1 - x, c], turns_ref.at[z, 1 - x, c])
        else:
            view = (keys_ref.at[flip(z, d), :, c], turns_ref.at[flip(z, d), :, c])
        return key_pair(view, kc_send, kc_recv, d, at_c)

    def a_copy(yy):
        return remote(
            mixed_ref.at[yy * 2 + 1 - c], mixed_in.at[yy], a_send.at[yy], a_recv.at[yy], at_c
        )

    def j_copy():
        return remote(joint_send, joint_recv, j_send.at[0], j_recv.at[0], at_y)

    started = []

    def copies_of(maker, args):
        made = maker(*args)
        return made if isinstance(made, list) else [made]

    def start(maker, *args):
        for copy in copies_of(maker, args):
            copy.start()
        if (maker, args) not in started:
            started.append((maker, args))

    def arrive(maker, *args):
        for copy in copies_of(maker, args):
            copy.wait_recv()

    def scale_of(group_index):
        table = dot(order_ref[group_lines(group_index), :], scale_ref[...])
        return jnp.sum(table, axis=-1, keepdims=True)

    def permuted(group_index, scale, first_col, cols):
        place_of = pl.ds(pl.multiple_of(first_col, 128), cols)
        picked = dot(order_ref[group_lines(group_index), :], tokens_ref[:, place_of])
        return (picked * scale * gain_ref[:, place_of]).astype(jnp.bfloat16)

    def make_units(d):
        eighths = min(Z_SPARES[d * HALVES + h] for h in range(HALVES))
        spare = half * eighths // 8
        outgoing_ref[flip(z, d), :, sides(eighths)[0]] = permuted(
            flip(z, d), scale_of(flip(z, d)), c * half + y * spare, half - spare
        )

    def make_own():
        scale = scale_of(z)
        for part in range(2):
            member_ref[part, z, x] = permuted(z, scale, part * half, half)

    made = set()
    for u in SENDS:
        d = u // HALVES
        if d not in made:
            if d > 0:
                make_units(d)
            else:
                make_own()
            if not made:
                pl.semaphore_wait(barrier, 6)
            made.add(d)
        if d > 0:
            start(z_copy, u)
        else:
            start(x_copy, u)

    def send_weights():
        loads["share"].wait()
        first_is_even = picks_even(route_ref[0:1, :])
        even = jnp.where(first_is_even, share_ref[0:1, :], share_ref[1:2, :])
        odd = jnp.where(first_is_even, share_ref[1:2, :], share_ref[0:1, :])
        line = iota((8, tok_rows), 0)
        table = jnp.zeros((8, tok_rows), jnp.float32)
        for k, value in enumerate(split(even) + split(odd)):
            table = jnp.where(line == k, jnp.broadcast_to(value, table.shape), table)
        table = table.astype(jnp.bfloat16)
        for g in range(GROUPS):
            weight_ref[g] = dot_lanes(table, order_ref[g * rows : (g + 1) * rows, :])
        for d in (1, 3, 2):
            start(w_copy, d)

    def picks_even(chosen):
        odd = jnp.zeros(chosen.shape, jnp.bool_)
        for e in range(1, GROUPS * TOPK, TOPK):
            odd = odd | (chosen == e)
        return jnp.logical_not(odd)

    def set_columns(d):
        if d > 0:
            arrive(w_copy, d)
        tile = weight_ref[z] if d == 0 else weight_in[flip(z, d)]
        even = tile[0:1] + tile[1:2] + tile[2:3]
        odd = tile[3:4] + tile[4:5] + tile[5:6]
        for k, line in enumerate(
            (jnp.where(x == 0, even, odd), jnp.where(x == 0, odd, even))
        ):
            column_ref[d, k] = jnp.transpose(jnp.broadcast_to(line, (rows, rows)))

    attend_rows, rank = latent_ref.shape
    key_half = attend_rows // 2
    lanes = 2 * ROPE

    def tables():
        lane = iota((1, lanes), 1)
        pair = (lane & (ROPE - 1)) >> 1
        quarter = ROPE // 4
        inverse = jnp.zeros((1, lanes), jnp.float32)
        for j in range(quarter):
            rate = rotary_base ** (-2.0 * j / (ROPE // 2))
            inverse = jnp.where((pair & (quarter - 1)) == j, rate, inverse)
        position = (ep * attend_rows + iota((attend_rows, lanes), 0)).astype(jnp.float32)
        grid_row = jnp.floor(position * (1.0 / GRID_W))
        grid_col = position - grid_row * GRID_W
        angle = jnp.where(jnp.broadcast_to(pair, position.shape) < quarter, grid_row, grid_col)
        angle = angle * inverse
        return jnp.cos(angle), jnp.sin(angle)

    def swap_matrix():
        from_lane = iota((lanes, lanes), 0)
        to_lane = iota((lanes, lanes), 1)
        to_even = (to_lane & 1) == 0
        swap = jnp.where(to_even & (from_lane == to_lane + 1), -1.0, 0.0)
        swap = jnp.where(jnp.logical_not(to_even) & (from_lane == to_lane - 1), 1.0, swap)
        return swap.astype(jnp.bfloat16)

    def make_keys():
        cosine, sine = tables()
        swap = swap_matrix()
        low_lane = iota((key_half, lanes), 1) < ROPE
        for name in ("key_gain", "latent", "rope"):
            loads[name].wait()
        keys_ref[z, x] = scaled(latent_ref[...], key_gain_ref[...]).reshape(2, key_half, rank)
        twice = jnp.transpose(jnp.concatenate([wide(rope_ref[...])] * 2, axis=0))
        turned = twice * cosine + dot(twice.astype(jnp.bfloat16), swap) * sine
        packed = jnp.where(low_lane, turned[:key_half], turned[key_half:])
        turns_ref[z, x] = packed.astype(jnp.bfloat16).reshape(2, key_half // 2, lanes)
        start(kx_copy, 0)
        for d in (1, 3, 2):
            start(kz_copy, d)
        for name in ("query_gain", "query", "w_query", "w_rope"):
            loads[name].wait()
        query_normed = scaled(query_ref[...], query_gain_ref[...])
        query_nope_ref[...] = dot(query_normed, w_query_ref[...]).astype(jnp.bfloat16)
        swapped = dot(w_rope_ref[...], swap).astype(jnp.bfloat16)
        query_turn = dot(query_normed, w_rope_ref[...]) * cosine
        query_turn = query_turn + dot(query_normed, swapped) * sine
        low = iota((attend_rows, lanes), 1) < ROPE
        for head in range(2):
            own = jnp.where(low if head == 0 else jnp.logical_not(low), query_turn, 0.0)
            other = pltpu.roll(own, ROPE, 1)
            query_turn_ref[head, head] = own.astype(jnp.bfloat16)
            query_turn_ref[head, 1 - head] = other.astype(jnp.bfloat16)

    def make_back():
        for k in range(tok_rows // rows):
            spread = jnp.broadcast_to(wide(place[:, k * rows : (k + 1) * rows]), (rows, rows))
            spread = jnp.transpose(spread)
            for g in range(GROUPS):
                target = (iota((rows, rows), 1) + g * rows).astype(jnp.float32)
                hit = jnp.where(spread == target, 1.0, 0.0).astype(jnp.bfloat16)
                back_ref[g, k * rows : (k + 1) * rows, :] = hit

    def compute(u):
        low = member_ref[0, block_at(u), :, lines_at(u), :].reshape(2 * lines_of, half)
        high = member_ref[1, block_at(u), :, lines_at(u), :].reshape(2 * lines_of, half)

        def project(weights):
            return dot(low, weights[:half, :]) + dot(high, weights[half:, :])

        gate_act = project(gate_ref)
        up_act = project(up_ref)
        hidden = (gate_act / (1.0 + jnp.exp(-gate_act)) * up_act).astype(jnp.bfloat16)
        for yy in range(2):
            term = dot(hidden, down_ref[yy * 2 + 1 - c])
            pair_send[u, yy] = term.astype(jnp.bfloat16).reshape(2, lines_of, share)
        start(p_copy, u)
        for yy in range(2):
            term = dot(hidden, down_ref[yy * 2 + c])
            pair_keep[u, yy] = term.astype(jnp.bfloat16).reshape(2, lines_of, share)

    def weights_of(u):
        def columns(k):
            square = column_ref[u // HALVES, k, lines_at(u), :]
            return jnp.concatenate([square] * (share // rows), axis=1)

        return columns(0), columns(1)

    def attend():
        for name in ("w_key", "w_value", "w_out"):
            loads[name].wait()
        blocks = keys_ref.shape[0] * keys_ref.shape[1]
        latents = keys_ref[...].reshape(blocks * attend_rows, rank)
        turns = turns_ref[...].reshape(blocks * key_half, lanes)
        key_nope = dot(latents, w_key_ref[...]).astype(jnp.bfloat16)
        value_rows = dot(latents, w_value_ref[...]).astype(jnp.bfloat16)
        key_nope = key_nope.reshape(blocks, 2, key_half, key_nope.shape[1])
        value_rows = value_rows.reshape(blocks, 2, key_half, value_rows.shape[1])
        for head in range(w_query_ref.shape[1] // NOPE):
            own = slice(head * NOPE, (head + 1) * NOPE)
            scores = []
            for part in range(2):
                left = jnp.concatenate(
                    [query_nope_ref[:, own], query_turn_ref[head, part]], axis=1
                )
                keys = key_nope[:, part, :, own].reshape(blocks * key_half, NOPE)
                right = jnp.concatenate([keys, turns], axis=1)
                scores.append(dot_lanes(left, right) * (NOPE + ROPE) ** (-0.5))
            top = jnp.maximum(
                jnp.max(scores[0], axis=-1, keepdims=True),
                jnp.max(scores[1], axis=-1, keepdims=True),
            )
            totals = jnp.zeros(top.shape, jnp.float32)
            mixed = jnp.zeros((attend_rows, VDIM), jnp.float32)
            for part in range(2):
                raised = jnp.exp(scores[part] - top)
                totals = totals + jnp.sum(raised, axis=-1, keepdims=True)
                values = value_rows[:, part, :, own].reshape(blocks * key_half, VDIM)
                mixed = mixed + dot(raised.astype(jnp.bfloat16), values)
            heads_ref[:, own] = (mixed / totals).astype(jnp.bfloat16)
        for t in range(4):
            lines = slice(t * (attend_rows // 4), (t + 1) * (attend_rows // 4))
            mixed_ref[t] = dot(heads_ref[lines, :], w_out_ref[...]).astype(jnp.bfloat16)
        for yy in range(2):
            start(a_copy, yy)

    def attend_join():
        for yy in range(2):
            arrive(a_copy, yy)
        sums = wide(mixed_ref[(1 - y) * 2 + c]) + wide(mixed_in[1 - y])
        joint_send[...] = sums.astype(jnp.bfloat16)
        start(j_copy)

    def attend_last():
        arrive(j_copy)
        sums = wide(mixed_ref[y * 2 + c]) + wide(mixed_in[y]) + wide(joint_recv[...])
        mixer_ref[...] = sums.astype(jnp.bfloat16)

    def stage_first(u):
        arrive(p_copy, u)
        if x_leads(u):
            for yy in range(2):
                sums = wide(pair_keep[u, yy, 1 - x]) + wide(pair_recv[u, yy, 1 - x])
                first_send[u, yy] = sums.astype(jnp.bfloat16)
            start(f_copy, u)
            for yy in range(2):
                first_keep[u, yy] = wide(pair_keep[u, yy, x]) + wide(pair_recv[u, yy, x])
        else:
            for line in range(2):
                sums = wide(pair_keep[u, 1 - y, line]) + wide(pair_recv[u, 1 - y, line])
                first_send[u, line] = sums.astype(jnp.bfloat16)
            start(f_copy, u)
            for line in range(2):
                first_keep[u, line] = wide(pair_keep[u, y, line]) + wide(pair_recv[u, y, line])

    def stage_second(u):
        arrive(f_copy, u)
        if x_leads(u):
            mine, other = weights_of(u)
            sums = mine * first_keep[u, 1 - y] + other * wide(first_recv[u, 1 - y])
            second_send[u] = sums.astype(jnp.bfloat16)
            start(s_copy, u)
            second_keep[u] = mine * first_keep[u, y] + other * wide(first_recv[u, y])
        else:
            sums = first_keep[u, 1 - x] + wide(first_recv[u, 1 - x])
            second_send[u] = sums.astype(jnp.bfloat16)
            start(s_copy, u)
            sums = first_keep[u, x] + wide(first_recv[u, x])
            second_keep[u] = wide(sums.astype(jnp.bfloat16))

    def stage_last(u):
        arrive(s_copy, u)
        if x_leads(u):
            result = second_keep[u] + wide(second_recv[u])
        else:
            mine, other = weights_of(u)
            result = mine * second_keep[u] + other * wide(second_recv[u])
        if u // HALVES == 0:
            fin_ref[z, lines_at(u)] = result.astype(jnp.bfloat16)
        else:
            fin_send[u] = result.astype(jnp.bfloat16)
            start(o_copy, u)

    def from_z(u):
        arrive(z_copy, u)
        start(x_copy, u)
        if Z_SPARES[u] > 0:
            start(y_copy, u, 0)

    def from_x(u):
        arrive(x_copy, u)
        start(y_copy, u, 1)

    def from_y(u, rel):
        if rel == 1 or Z_SPARES[u] > 0:
            arrive(y_copy, u, rel)
        start(c_copy, u, rel)

    def gathered(u):
        for rel in range(2):
            if u // HALVES > 0 or rel > 0:
                arrive(c_copy, u, rel)

    def wait_weights():
        for name in ("gate", "up"):
            loads[name].wait()
        for t in range(4):
            loads[("down", t)].wait()

    def from_kz(d):
        arrive(kz_copy, d)
        start(kx_copy, d)

    def from_kx(d):
        arrive(kx_copy, d)
        start(kc_copy, d)

    def from_kc(d):
        arrive(kc_copy, d)

    added = []

    def give_back(d):
        if d > 0:
            for h in range(HALVES):
                arrive(o_copy, d * HALVES + h)
        term = dot(back_ref[flip(z, d)], fin_ref[flip(z, d)])
        if added:
            term = term + wide(moe_ref[...])
        added.append(d)
        moe_ref[...] = term.astype(jnp.bfloat16)

    steps = {
        "z": from_z,
        "x": from_x,
        "y": from_y,
        "g": gathered,
        "m": compute,
        "1": stage_first,
        "2": stage_second,
        "3": stage_last,
        "weights": send_weights,
        "columns": set_columns,
        "keys": make_keys,
        "back": make_back,
        "loaded": wait_weights,
        "kz": from_kz,
        "kx": from_kx,
        "kc": from_kc,
        "attend": attend,
        "join": attend_join,
        "last": attend_last,
        "b": give_back,
    }

    for item in SCHEDULE:
            where, text = "", item
            if item[0] in "<>":
                where, text = item[0], item[1:]
            name, *numbers = text.split(".")
            step = steps[name]
            values = [int(number) for number in numbers]
            if where == "":
                step(*values)
            else:
                pl.when(at_end if where == ">" else jnp.logical_not(at_end))(
                    functools.partial(step, *values)
                )
    for maker, args in started:
        for copy in copies_of(maker, args):
            copy.wait_send()


SCHEDULE = (
    "keys", "loaded", "<z.2", "<z.6", "x.0", "<z.7", "<x.1", "<x.2", "<y.7.0", "z.3", "<x.6",
    "y.0.1", ">x.1", ">z.6", ">z.2", "<x.7", "<y.2.1", "<y.6.0", "x.3", ">x.6", ">kz.1", ">z.7",
    "<y.6.1", "z.4", ">x.7", ">y.6.1", ">y.7.0", ">y.6.0", "<y.7.1", "z.5", "g.0", "m.0", ">y.3.1",
    ">x.4", "g.6", "m.6", ">y.7.1", "<kz.1", "<y.4.0", "<x.4", "weights", "<kz.3", "<y.3.1",
    "<y.3.0", "x.5", ">y.3.0", ">kz.2", "<y.2.0", "1.6", ">kx.1", "g.7", "m.7", ">x.2", "<y.5.0",
    "g.3", "m.3", ">kx.2", "<y.1.1", "1.7", ">y.5.0", ">y.4.0", ">kz.3", "y.5.1", ">y.2.0", "y.4.1",
    "1.3", "columns.3", "g.5", "m.5", ">kc.2", "2.6", "columns.1", ">y.2.1", "<kx.3", "1.5",
    ">kx.3", "<kx.1", "g.4", "m.4", "columns.0", "<kc.3", "2.7", "g.2", "m.2", ">kx.0", "<kz.2",
    "<kc.1", "3.6", "2.3", "1.4", "columns.2", "<kx.0", "1.2", ">y.1.1", "<kc.0", "3.7", ">kc.3",
    ">kc.1", "<kx.2", "g.1", "m.1", "2.5", "1.0", ">kc.0", "3.3", "<kc.2", "attend", "2.2", "1.1",
    "3.5", "2.4", "join", "3.2", "3.4", "2.0", "back", "b.3", "2.1", "last", "3.0", "b.1", "3.1",
    "b.0", "b.2",
)


def expert_exchange(tokens_b, ffn_gain, route, share_of, w_gate, w_up, w_down, mixer_args):
    tok_rows, width = tokens_b.shape
    rows = tok_rows // GROUPS
    half = width // 2
    share = width // 4
    units = w_gate.shape[2]
    attend_rows, rank = mixer_args[1].shape
    head_cols = mixer_args[7].shape[1]
    rank_q = mixer_args[0].shape[1]
    count = GROUPS * HALVES
    part = rows // HALVES
    narrow, full = jnp.bfloat16, jnp.float32
    vmem = pl.BlockSpec(memory_space=pltpu.VMEM)
    anywhere = pl.BlockSpec(memory_space=pl.ANY)
    dma = pltpu.SemaphoreType.DMA
    operands = (
        tokens_b,
        ffn_gain.reshape(1, width),
        route,
        share_of,
        w_gate,
        w_up,
        w_down,
        *mixer_args,
    )
    return pl.pallas_call(
        expert_kernel,
        out_shape=(
            pltpu.VMEM((tok_rows, share), narrow),
            pltpu.VMEM((attend_rows // 4, width), narrow),
        ),
        in_specs=[anywhere] * len(operands),
        out_specs=(vmem, vmem),
        scratch_shapes=[
            pltpu.VMEM((tok_rows, width), narrow),
            pltpu.VMEM((1, width), full),
            pltpu.VMEM(route.shape, jnp.int32),
            pltpu.VMEM(share_of.shape, full),
            pltpu.VMEM((attend_rows, rank_q), narrow),
            pltpu.VMEM((attend_rows, rank), narrow),
            pltpu.VMEM((ROPE, attend_rows), narrow),
            pltpu.VMEM((1, rank_q), full),
            pltpu.VMEM((1, rank), full),
            pltpu.VMEM(mixer_args[5].shape, narrow),
            pltpu.VMEM(mixer_args[6].shape, narrow),
            pltpu.VMEM(mixer_args[7].shape, narrow),
            pltpu.VMEM(mixer_args[8].shape, narrow),
            pltpu.VMEM(mixer_args[9].shape, narrow),
            pltpu.VMEM((tok_rows, tok_rows), narrow),
            pltpu.VMEM((GROUPS, tok_rows, rows), narrow),
            pltpu.VMEM((GROUPS, 8, rows), full),
            pltpu.VMEM((GROUPS, 8, rows), full),
            pltpu.VMEM((GROUPS, 2, rows, rows), full),
            pltpu.VMEM((tok_rows, 128), narrow),
            pltpu.VMEM((GROUPS, rows, half), narrow),
            pltpu.VMEM((2, GROUPS, 2, rows, half), narrow),
            pltpu.VMEM((width, units), narrow),
            pltpu.VMEM((width, units), narrow),
            pltpu.VMEM((4, units, share), narrow),
            pltpu.VMEM((count, 2, 2, part, share), narrow),
            pltpu.VMEM((count, 2, 2, part, share), narrow),
            pltpu.VMEM((count, 2, 2, part, share), narrow),
            pltpu.VMEM((count, 2, part, share), narrow),
            pltpu.VMEM((count, 2, part, share), full),
            pltpu.VMEM((count, 2, part, share), narrow),
            pltpu.VMEM((count, part, share), narrow),
            pltpu.VMEM((count, part, share), full),
            pltpu.VMEM((count, part, share), narrow),
            pltpu.VMEM((count, part, share), narrow),
            pltpu.VMEM((GROUPS, rows, share), narrow),
            pltpu.VMEM((GROUPS, 2, 2, attend_rows // 2, rank), narrow),
            pltpu.VMEM((GROUPS, 2, 2, attend_rows // 4, 2 * ROPE), narrow),
            pltpu.VMEM((attend_rows, head_cols), narrow),
            pltpu.VMEM((2, 2, attend_rows, 2 * ROPE), narrow),
            pltpu.VMEM((attend_rows, head_cols), narrow),
            pltpu.VMEM((4, attend_rows // 4, width), narrow),
            pltpu.VMEM((2, attend_rows // 4, width), narrow),
            pltpu.VMEM((attend_rows // 4, width), narrow),
            pltpu.VMEM((attend_rows // 4, width), narrow),
            dma((4,)),
            dma((24,)),
        ]
        + [dma((count,))] * 4
        + [dma((2 * count,))] * 4
        + [dma((count,))] * 8
        + [dma((GROUPS,))] * 2
        + [dma((2 * GROUPS,))] * 6
        + [dma((2,))] * 4,
        compiler_params=pltpu.CompilerParams(
            collective_id=0, has_side_effects=True, vmem_limit_bytes=48 * 1024 * 1024
        ),
        cost_estimate=pl.CostEstimate(
            flops=40_000_000_000, bytes_accessed=8_000_000, transcendentals=0
        ),
        name="expert_exchange",
    )(*(pltpu.with_memory_space_constraint(operand, pltpu.HBM) for operand in operands))


def paired(mixer, tokens_b, ffn_gain, route_expert, route_weight, w_gate, w_up, w_down):
    query_latent, key_latent, rope_key, query_gain, key_gain = mixer[:5]
    mixer_args = (
        query_latent,
        key_latent,
        rope_key.T,
        query_gain.reshape(1, -1),
        key_gain.reshape(1, -1),
        *mixer[5:],
    )
    moe_out, mixer_out = expert_exchange(
        tokens_b, ffn_gain, route_expert.T, route_weight.T, w_gate, w_up, w_down, mixer_args
    )
    return (mixer_out, moe_out)


def body(
    query_latent,
    key_latent,
    rope_key,
    query_gain,
    key_gain,
    w_query,
    w_query_rope,
    w_key,
    w_value,
    w_out,
    tokens_b,
    ffn_gain,
    route_expert,
    route_weight,
    w_gate,
    w_up,
    w_down,
):
    mixer = (
        query_latent,
        key_latent,
        rope_key,
        query_gain,
        key_gain,
        w_query,
        w_query_rope,
        w_key,
        w_value,
        w_out,
    )
    experts = (tokens_b, ffn_gain, route_expert, route_weight, w_gate, w_up, w_down)
    if (
        lax.axis_size("ep") == GROUPS * TOPK
        and lax.axis_size("tp") == 4
        and GROUPS == 4
        and tokens_b.shape[0] == GROUPS * 128
        and w_query.shape[1] == 2 * NOPE
    ):
        return paired(mixer, *experts)
    return (mixer_half(*mixer), expert_half(*experts))


def solution(mesh):
    in_specs = (
        P("ep", None),
        P("ep", None),
        P("ep", None),
        P(),
        P(),
        P(None, "tp"),
        P(None, "tp"),
        P(None, "tp"),
        P(None, "tp"),
        P("tp", None),
        P("ep", None),
        P(),
        P("ep", None),
        P("ep", None),
        P("ep", None, "tp"),
        P("ep", None, "tp"),
        P("ep", "tp", None),
    )
    out_specs = (P(("ep", "tp"), None), P("ep", "tp"))
    return jax.shard_map(body, mesh=mesh, in_specs=in_specs, out_specs=out_specs, check_vma=False)
```
